256 devices in a mesh: grp: 2 (over z), kv: 16 (over y, core), tp: 8 (over x).
Axes of the slice: x: 8, y: 8, z: 2, core: 2. Of those that a mesh axis runs over, the one named last changes fastest.
The devices are a block of a 8x8x16 slice.
Arguments:
- tokens: bfloat16 [512, 4096], P('grp', ('kv', 'tp')), parts along dimension 0, may hold values from -20 to 20, as said below
- norm_gain: bfloat16 [4096], P('kv'), may hold values from 0.099609375 to 1.8984375
- w_query: bfloat16 [4096, 2048], P('kv', 'tp'), may hold values from -0.09375 to 0.09375
- w_key: bfloat16 [4096, 2048], P('kv', 'tp'), may hold values from -0.09375 to 0.09375
- w_value: bfloat16 [4096, 4096], P('kv', 'tp'), may hold values from -0.09375 to 0.09375
- w_outgate: bfloat16 [4096, 4096], P('kv', 'tp'), may hold values from -0.09375 to 0.09375
- w_input_gate: bfloat16 [4096, 32], P('kv'), may hold values from -0.09375 to 0.09375
- w_forget_gate: bfloat16 [4096, 32], P('kv'), may hold values from -0.09375 to 0.09375
- memory: float32 [512, 32, 64, 128], P(('grp', 'kv'), 'tp'), parts along dimension 0, may hold values from -4 to 4
- normalizer: float32 [512, 32, 64], P(('grp', 'kv'), 'tp'), parts along dimension 0, may hold values from -4 to 4
- stabilizer: float32 [512, 32], P(('grp', 'kv'), 'tp'), parts along dimension 0, may hold values from -4 to 4
- w_mix_out: bfloat16 [4096, 4096], P('tp', 'kv'), may hold values from -0.09375 to 0.09375
- ffn_gain: bfloat16 [4096], P('kv'), may hold values from 0.099609375 to 1.8984375
- w_gate: bfloat16 [4096, 11264], P('kv', 'tp'), may hold values from -0.09375 to 0.09375
- w_up: bfloat16 [4096, 11264], P('kv', 'tp'), may hold values from -0.09375 to 0.09375
- w_down: bfloat16 [11264, 4096], P('tp', 'kv'), may hold values from -0.3125 to 0.3125
Outputs:
- layer_out: bfloat16 [512, 4096], P('grp', ('kv', 'tp')), parts along dimension 0
- new_memory: float32 [512, 32, 64, 128], P(('grp', 'kv'), 'tp'), parts along dimension 0
- new_normalizer: float32 [512, 32, 64], P(('grp', 'kv'), 'tp'), parts along dimension 0
- new_stabilizer: float32 [512, 32], P(('grp', 'kv'), 'tp'), parts along dimension 0
The draws below stay inside these ranges and needn't reach their ends.
There are 2 independent parts, one for each index of `grp`. The reference program is written for one: setup_inputs(seed, part) draws one part's arguments, and reference() takes and returns one part's arrays. A program takes and returns all parts, laid end to end along the dimension named above; an argument that names none is the same for every part. Nothing has to cross between parts.
Inputs may be any that keep to these rules, and one draw needn't show every extreme that they name: tokens' feature scales differ by column and by sequence.
All inputs are finite; a program needn't handle non-finite values.
Results may differ from the reference program's by a relative error of at most 0.029.
Values may be sent and summed in bfloat16 or wider, within the bound.
A program may use at most 64 MiB of HBM per device.

```python
import jax
import jax.numpy as jnp
from jax import lax

D = 4096
NH = 32
DQK = 64
DV = 128
FF = 11264
SEQS = 256
N_TP = 8


def draw_tokens(key, part):
    base_key, col_key, row_key = jax.random.split(jax.random.fold_in(key, 11), 3)
    columns = jnp.arange(D, dtype=jnp.float32) / (D - 1)
    col_scale = 0.1 * 10.0 ** columns * jax.random.uniform(col_key, (D,), jnp.float32, 0.7, 1.3)
    row_factor = 10.0 ** (jax.random.uniform(row_key, (SEQS, 1), jnp.float32) - 0.5)
    base = jnp.clip(jax.random.normal(base_key, (SEQS, D), jnp.float32), -4.0, 4.0)
    return (base * col_scale[None, :] * row_factor).astype(jnp.bfloat16)


def draw_stabilizer(key, part):
    base_key = jax.random.fold_in(jax.random.fold_in(key, 23), 0)
    base = jax.random.uniform(base_key, (SEQS, NH), jnp.float32, -4.0, 4.0)
    return base


def raised(array, key, source, target, parts, factor):
    def block_of(position):
        return (jnp.arange(array.shape[position]) // (array.shape[position] // parts)).reshape((-1,) + (1,) * (array.ndim - 1 - position))

    near = jax.random.permutation(key, parts)[block_of(target)]
    second = (block_of(target) + parts // 2) % parts
    return jnp.where((block_of(source) == near) | (block_of(source) == second), factor * array, array)


def block_scale(own_key, extent, shards, least, top_value):
    def one(position, shards_of):
        steps = jax.random.uniform(jax.random.fold_in(jax.random.fold_in(own_key, 6), position), (shards_of,), jnp.float32, least / len(shards), top_value / len(shards))
        return jnp.repeat(jnp.exp(steps), extent[position] // shards_of).reshape((-1,) + (1,) * (len(extent) - position - 1))

    gain = one(*shards[0])
    for cut in shards[1:]:
        gain = gain * one(*cut)
    return gain


def gaussian(rng, shape, spread, most, cuts=(), kind=jnp.bfloat16):
    result = spread * jax.random.normal(rng, shape, jnp.float32)
    if cuts:
        result = result * block_scale(rng, shape, cuts, -0.22, 0.18)
    return jnp.clip(result, -most, most).astype(kind)


def noise_with(key, shape, deviation, most, cuts, heavy, kind=jnp.bfloat16):
    array = deviation * jax.random.normal(key, shape, jnp.float32)
    if cuts:
        array = array * block_scale(key, shape, cuts, -0.22, 0.18)
    return jnp.clip(raised(array, jax.random.fold_in(key, 3), *heavy), -most, most).astype(kind)


def setup_inputs(seed: int = 0, part: int = 0) -> dict:
    key_of = jax.random.split(jax.random.key(seed), 17)
    part_keys = jax.random.split(jax.random.fold_in(key_of[16], part), 17)
    return {
        "tokens": draw_tokens(jax.random.fold_in(jax.random.fold_in(key_of[16], part), 71), part),
        "norm_gain": jnp.clip(1.0 + 0.18 * jax.random.normal(key_of[1], (D,), jnp.float32), 0.099609375, 1.8984375).astype(jnp.bfloat16),
        "w_query": gaussian(key_of[2], (D, NH * DQK), D ** -0.5, 0.09375, ((0, 16), (1, 8))),
        "w_key": gaussian(key_of[3], (D, NH * DQK), D ** -0.5, 0.09375, ((0, 16), (1, 8))),
        "w_value": gaussian(key_of[4], (D, NH * DV), D ** -0.5, 0.09375, ((0, 16), (1, 8))),
        "w_outgate": gaussian(key_of[5], (D, NH * DV), D ** -0.5, 0.09375, ((0, 16), (1, 8))),
        "w_input_gate": gaussian(key_of[6], (D, NH), D ** -0.5, 0.09375, ((0, 16),)),
        "w_forget_gate": gaussian(key_of[7], (D, NH), D ** -0.5, 0.09375, ((0, 16),)),
        "memory": gaussian(part_keys[8], (SEQS, NH, DQK, DV), 0.5, 4.0, ((0, 16), (1, 8)), jnp.float32),
        "normalizer": gaussian(part_keys[9], (SEQS, NH, DQK), 0.5, 4.0, ((0, 16), (1, 8)), jnp.float32),
        "stabilizer": draw_stabilizer(jax.random.fold_in(jax.random.fold_in(key_of[16], part), 71), part),
        "w_mix_out": gaussian(key_of[11], (NH * DV, D), (NH * DV) ** -0.5, 0.09375, ((0, 8), (1, 16))),
        "ffn_gain": jnp.clip(1.0 + 0.18 * jax.random.normal(key_of[12], (D,), jnp.float32), 0.099609375, 1.8984375).astype(jnp.bfloat16),
        "w_gate": gaussian(key_of[13], (D, FF), D ** -0.5, 0.09375, ((0, 16), (1, 8))),
        "w_up": gaussian(key_of[14], (D, FF), D ** -0.5, 0.09375, ((0, 16), (1, 8))),
        "w_down": noise_with(key_of[15], (FF, D), (FF // 16) ** -0.5, 0.3125, ((0, 8), (1, 16)), (0, 1, 16, 2.0)),
    }


def row_scale(values):
    wide = values.astype(jnp.float32)
    return lax.rsqrt(lax.optimization_barrier(jnp.mean(wide * wide, axis=-1, keepdims=True)) + 1e-06)

def block_sum(left, right, blocks):
    rows = left.shape[0]
    inner = left.shape[1] // blocks
    left_b = left.reshape(rows, blocks, inner).transpose(1, 0, 2)
    right_b = right.reshape(blocks, inner, right.shape[1])

    def one_block(pair):
        partial_value = jnp.dot(pair[0], pair[1], preferred_element_type=jnp.float32)
        return partial_value.astype(jnp.bfloat16).astype(jnp.float32)
    return lax.optimization_barrier(jnp.sum(lax.map(one_block, (left_b, right_b)), axis=0))

def reference(tokens, norm_gain, w_query, w_key, w_value, w_outgate, w_input_gate, w_forget_gate, memory, normalizer, stabilizer, w_mix_out, ffn_gain, w_gate, w_up, w_down):
    seqs = tokens.shape[0]
    scale1 = row_scale(tokens)
    normed1 = (tokens.astype(jnp.float32) * norm_gain.astype(jnp.float32)).astype(jnp.bfloat16)

    def project(weight):
        return scale1 * jnp.dot(normed1, weight, preferred_element_type=jnp.float32)
    query = project(w_query).reshape(seqs, NH, DQK) * DQK ** (-0.5)
    key = project(w_key).reshape(seqs, NH, DQK)
    value = project(w_value).reshape(seqs, NH, DV)
    outgate = project(w_outgate)
    igate = project(w_input_gate)
    lforget = jax.nn.log_sigmoid(project(w_forget_gate))
    new_stabilizer = jnp.maximum(lforget + stabilizer, igate)
    decay = jnp.exp(lforget + stabilizer - new_stabilizer)
    inflow = jnp.exp(igate - new_stabilizer)
    new_memory = decay[:, :, None, None] * memory + inflow[:, :, None, None] * key[:, :, :, None] * value[:, :, None, :]
    new_normalizer = decay[:, :, None] * normalizer + inflow[:, :, None] * key
    numer = jnp.einsum('bhd,bhde->bhe', query, new_memory)
    denom = lax.optimization_barrier(jnp.sum(query * new_normalizer, axis=-1))
    readout = numer / jnp.maximum(jnp.abs(denom), jnp.exp(-new_stabilizer))[:, :, None]
    gated = (jax.nn.sigmoid(outgate) * readout.reshape(seqs, NH * DV)).astype(jnp.bfloat16)
    mixed_in = (tokens.astype(jnp.float32) + block_sum(gated, w_mix_out, N_TP)).astype(jnp.bfloat16)
    scale2 = row_scale(mixed_in)
    normed2 = (mixed_in.astype(jnp.float32) * ffn_gain.astype(jnp.float32)).astype(jnp.bfloat16)
    gate_pre = scale2 * jnp.dot(normed2, w_gate, preferred_element_type=jnp.float32)
    up_pre = scale2 * jnp.dot(normed2, w_up, preferred_element_type=jnp.float32)
    hidden = (jax.nn.silu(gate_pre) * up_pre).astype(jnp.bfloat16)
    layer_out = (mixed_in.astype(jnp.float32) + block_sum(hidden, w_down, N_TP)).astype(jnp.bfloat16)
    return (layer_out, new_memory, new_normalizer, new_stabilizer)
```

```python
import functools

import jax
import jax.numpy as jnp
from jax import lax
from jax.experimental import pallas as pl
from jax.experimental.pallas import tpu as pltpu
from jax.sharding import PartitionSpec as P

DQK = 64
DV = 128
LANES = 128
HALF = LANES // 2
F32 = jnp.float32
BF16 = jnp.bfloat16
MESH = pl.DeviceIdType.MESH


def far_first(count):
    return sorted(range(1, count), key=lambda d: -min(d, count - d))


def near_first(count):
    return far_first(count)[::-1]


def column_pieces(width, step=256):
    return [(at, min(step, width - at)) for at in range(0, width, step)]


def hi_lo(values, lane):
    high = values.astype(BF16).astype(F32)
    return jnp.where(lane < HALF, high, values - high).astype(BF16)


def from_hi_lo(tile):
    return tile[:, :HALF] + tile[:, HALF:]


def layer_kernel(
    n_kv, n_tp,
    tokens_h, norm_gain, wq_h, wk_h, wv_h, wo_h, wi_h, wf_h, mem_h, norm_h, stab_h, wmix_h, ffn_gain, wg_h, wu_h, wd_h,
    out_ref, newmem_h, newnorm_ref, newstab_ref,
    tokens, w1, wgates, mem, norm, stab, wmix, wmix_t, w2, wd, wd_t,
    token_t, x_raw, z1_pair, z1_own, z1_got, z1_send, z1_recv,
    numer, gated, mix_send, mix_recv, mixed_t, z2_pair, z2_own, z2_got, z2_send, z2_recv, hidden, down_send, down_recv,
    local_sem, tok_s, tok_r, p1_s, p1_r, a_s, a_r, g_s, g_r, gf_s, gf_r, m_s, m_r, x_s, x_r, p2_s, p2_r, b_s, b_r, h_s, h_r, hf_s, hf_r, d_s, d_r,
):
    kv, tp = lax.axis_index("kv"), lax.axis_index("tp")
    n_y = n_kv // 2
    core, y = lax.rem(kv, 2), kv // 2
    other = 1 - core
    partner = 2 * y + other
    own = mem.shape[0]
    heads = mem.shape[1]
    feats = token_t.shape[0]
    mine = tokens.shape[1]
    half_rows = n_y * own
    n_feats = feats * n_kv

    def y_of(d):
        return lax.rem(y + d, n_y)

    def from_y(d):
        return lax.rem(y + n_y - d, n_y)

    def tp_of(d):
        return lax.rem(tp + d, n_tp)

    def from_tp(d):
        return lax.rem(tp + n_tp - d, n_tp)

    def rows(index, size):
        return pl.ds(pl.multiple_of(index * size, size), size)

    barrier = pltpu.get_barrier_semaphore()
    for d in far_first(n_tp):
        pl.semaphore_signal(barrier, inc=1, device_id={"tp": tp_of(d)}, device_id_type=MESH)
    for d in far_first(n_y):
        pl.semaphore_signal(barrier, inc=1, device_id={"kv": 2 * y_of(d) + core}, device_id_type=MESH)
    pl.semaphore_signal(barrier, inc=1, device_id={"kv": partner}, device_id_type=MESH)

    dq, dk, dv = wq_h.shape[1], wk_h.shape[1], wv_h.shape[1]
    n_main = dq + dk + 2 * dv
    n_ff = wg_h.shape[1]
    n_gate = wi_h.shape[1]
    loads = {}
    for i, (name, source, target) in enumerate((
        ("tokens", tokens_h, tokens),
        ("wi", wi_h, wgates.at[0]),
        ("wf", wf_h, wgates.at[1]),
        ("wq", wq_h, w1.at[:, pl.ds(0, dq)]),
        ("wk", wk_h, w1.at[:, pl.ds(dq, dk)]),
        ("wv", wv_h, w1.at[:, pl.ds(dq + dk, dv)]),
        ("wo", wo_h, w1.at[:, pl.ds(dq + dk + dv, dv)]),
        ("mix", wmix_h, wmix),
        ("down", wd_h, wd),
        ("mem", mem_h, mem),
        ("norm", norm_h, norm),
        ("stab", stab_h, stab),
        ("gate", wg_h, w2.at[:, pl.ds(0, n_ff)]),
        ("up", wu_h, w2.at[:, pl.ds(n_ff, n_ff)]),
    )):
        loads[name] = pltpu.make_async_copy(source, target, local_sem.at[i])
        loads[name].start()
    sent = []

    def send(source, target, send_sem, recv_sem, where):
        copy = pltpu.make_async_remote_copy(
            src_ref=source, dst_ref=target, send_sem=send_sem, recv_sem=recv_sem, device_id=where, device_id_type=MESH
        )
        copy.start()
        sent.append(copy)

    def arrive(target, send_sem, recv_sem, where):
        pltpu.make_async_remote_copy(
            src_ref=target, dst_ref=target, send_sem=send_sem, recv_sem=recv_sem, device_id=where, device_id_type=MESH
        ).wait_recv()

    loads["tokens"].wait()
    token_t[rows(tp, mine), :] = tokens[...].astype(F32).T.astype(BF16)
    pl.semaphore_wait(barrier, (n_tp - 1) + (n_y - 1) + 1)
    for d in far_first(n_tp):
        part = token_t.at[rows(tp, mine), :]
        send(part, part, tok_s.at[d], tok_r.at[d], {"tp": tp_of(d)})

    loads["wi"].wait()
    loads["wf"].wait()
    lane_w = lax.broadcasted_iota(jnp.int32, (n_gate, LANES), 1)
    row_w = lax.broadcasted_iota(jnp.int32, (n_gate, LANES), 0)
    low_lane = lax.rem(lane_w, HALF)
    head_row = row_w - tp * heads
    pick_i = jnp.where((low_lane == head_row) & (head_row < heads) & (head_row >= 0), 1.0, 0.0).astype(BF16)
    pick_f = jnp.where((low_lane == head_row + heads) & (head_row < heads) & (head_row >= 0), 1.0, 0.0).astype(BF16)
    w1[:, n_main:] = (
        jnp.dot(wgates[0], pick_i, preferred_element_type=F32) + jnp.dot(wgates[1], pick_f, preferred_element_type=F32)
    ).astype(BF16)

    loads["mix"].wait()
    wmix_t[...] = wmix[...].T
    loads["down"].wait()
    for at, width in column_pieces(wd.shape[0]):
        wd_t[:, at : at + width] = wd[at : at + width, :].T
    for name in ("wq", "wk", "wv", "wo"):
        loads[name].wait()

    for d in near_first(n_tp):
        arrive(token_t.at[rows(from_tp(d), mine), :], tok_s.at[d], tok_r.at[d], {"tp": tp_of(d)})

    lane = lax.broadcasted_iota(jnp.int32, (half_rows, LANES), 1)

    def project(gain, weights, widths, square_lane, gates, core_of, store):
        wide = x_raw[:, core_of].reshape(half_rows, feats).astype(F32)
        normed = (wide * gain[...].astype(F32)).astype(BF16)
        squares = jnp.sum(wide * wide, axis=1, keepdims=True)
        for at, width in widths:
            store(at, width, jnp.dot(normed, weights[:, at : at + width], preferred_element_type=F32))
        end = widths[-1][0] + widths[-1][1]
        tile = jnp.broadcast_to(squares, (half_rows, LANES))
        if gates:
            last = jnp.dot(normed, weights[:, end : end + LANES], preferred_element_type=F32)
            tile = jnp.where(lax.rem(lane, HALF) == square_lane, tile, last)
        store(end, LANES, tile)

    def reduce_over_kv(gain, weights, width, square_lane, gates, pair, own_z, got, out, into, sems, total_at):
        p_s, p_r, r_s, r_r = sems
        pieces = column_pieces(width)

        def to_partner(at, size, z):
            value = hi_lo(z, lane) if at == width else z.astype(BF16)
            pair[:, :, at : at + size] = value.reshape(n_y, own, size)

        def keep(at, size, z):
            own_z[:, :, at : at + size] = z.reshape(n_y, own, size)

        project(gain, weights, pieces, square_lane, gates, other, to_partner)
        send(pair, got, p_s, p_r, {"kv": partner})
        project(gain, weights, pieces, square_lane, gates, core, keep)
        arrive(got, p_s, p_r, {"kv": partner})
        small_lane = lax.broadcasted_iota(jnp.int32, (own, LANES), 1)
        for d in far_first(n_y) + [0]:
            at_y = y_of(d)
            for at, size in pieces + [(width, LANES)]:
                both = own_z[at_y, :, at : at + size]
                other_half = got[at_y, :, at : at + size].astype(F32)
                if at == width:
                    both = both + (other_half + jnp.concatenate([other_half[:, HALF:], other_half[:, :HALF]], axis=1))
                    if d:
                        both = hi_lo(both, small_lane)
                else:
                    both = both + other_half
                if d:
                    out[d, :, at : at + size] = both.astype(BF16)
                else:
                    total_at[:, at : at + size] = both
            if d:
                send(out.at[d], into.at[d], r_s.at[d], r_r.at[d], {"kv": 2 * at_y + core})
        for d in near_first(n_y):
            arrive(into.at[d], r_s.at[d], r_r.at[d], {"kv": 2 * y_of(d) + core})

    def total_of(total_at, into, at, size):
        value = total_at[:, at : at + size]
        for d in range(1, n_y):
            value = value + into[d, :, at : at + size].astype(F32)
        return value

    def tile_of(total_at, into, at):
        rest = into[1, :, at : at + LANES].astype(F32)
        for d in range(2, n_y):
            rest = rest + into[d, :, at : at + LANES].astype(F32)
        return total_at[:, at : at + HALF] + from_hi_lo(rest)

    def gather_over_kv(buffer, sems):
        r_s, r_r, f_s, f_r = sems
        part = buffer.at[rows(kv, own), :]
        for d in far_first(n_y):
            send(part, part, r_s.at[d], r_r.at[d], {"kv": 2 * y_of(d) + core})
        send(part, part, f_s.at[0], f_r.at[0], {"kv": partner})

        def finish():
            for d in near_first(n_y):
                got = buffer.at[rows(2 * from_y(d) + core, own), :]
                arrive(got, r_s.at[d], r_r.at[d], {"kv": 2 * y_of(d) + core})
                send(got, got, f_s.at[d], f_r.at[d], {"kv": partner})
            for d in [0] + near_first(n_y):
                arrive(buffer.at[rows(2 * from_y(d) + other, own), :], f_s.at[d], f_r.at[d], {"kv": partner})

        return finish

    def sum_over_tp(partial, out, into, sems):
        s, r = sems
        out[...] = partial.astype(BF16).reshape(n_tp, mine, partial.shape[1])
        for d in far_first(n_tp):
            send(out.at[tp_of(d)], into.at[d], s.at[d], r.at[d], {"tp": tp_of(d)})
        total = out[tp].astype(F32)
        for d in near_first(n_tp):
            arrive(into.at[d], s.at[d], r.at[d], {"tp": tp_of(d)})
            total = total + into[d].astype(F32)
        return total

    z_total = z1_own.at[y]
    x_raw[...] = token_t[...].T.reshape(x_raw.shape)
    reduce_over_kv(
        norm_gain, w1, n_main, 2 * heads, True, z1_pair, z1_own, z1_got, z1_send, z1_recv, (p1_s, p1_r, a_s, a_r), z_total
    )
    gates = tile_of(z_total, z1_recv, n_main)
    scale1 = lax.rsqrt(gates[:, 2 * heads : 2 * heads + 1] / n_feats + 1e-06)
    query = scale1 * total_of(z_total, z1_recv, 0, dq) * DQK ** (-0.5)
    key = scale1 * total_of(z_total, z1_recv, dq, dk)
    value = scale1 * total_of(z_total, z1_recv, dq + dk, dv)
    outgate = scale1 * total_of(z_total, z1_recv, dq + dk + dv, dv)
    igate = scale1 * gates[:, :heads]
    forget = scale1 * gates[:, heads : 2 * heads]
    lforget = jnp.minimum(forget, 0.0) - jnp.log1p(jnp.exp(-jnp.abs(forget)))
    loads["stab"].wait()
    loads["norm"].wait()
    loads["mem"].wait()
    held = lforget + stab[...]
    new_stab = jnp.maximum(held, igate)
    newstab_ref[...] = new_stab
    decay = jnp.exp(held - new_stab)
    inflow = jnp.exp(igate - new_stab)
    floor = jnp.exp(-new_stab)
    query_t = query.T
    for s in range(own):
        for h in range(heads):
            column = query_t[h * DQK : (h + 1) * DQK, s : s + 1]
            numer[s : s + 1, h * DV : (h + 1) * DV] = jnp.sum(column * mem[s, h], axis=0, keepdims=True)
    for h in range(heads):
        q, k = query[:, h * DQK : (h + 1) * DQK], key[:, h * DQK : (h + 1) * DQK]
        keep, add = decay[:, h : h + 1], inflow[:, h : h + 1]
        new_norm = keep * norm[:, h, :] + add * k
        newnorm_ref[:, h, :] = new_norm
        denom = jnp.maximum(jnp.abs(jnp.sum(q * new_norm, axis=1, keepdims=True)), floor[:, h : h + 1])
        at = slice(h * DV, (h + 1) * DV)
        top = keep * numer[:, at] + (add * jnp.sum(q * k, axis=1, keepdims=True)) * value[:, at]
        gated[rows(kv, own), at] = (jax.nn.sigmoid(outgate[:, at]) * (top / denom)).astype(BF16)
    finish = gather_over_kv(gated, (g_s, g_r, gf_s, gf_r))

    spread = jnp.concatenate([jnp.broadcast_to(inflow[:, h : h + 1], (own, DQK)) for h in range(heads)], axis=1)
    key_t = (key * spread).T
    for s in range(own):
        for h in range(heads):
            column = key_t[h * DQK : (h + 1) * DQK, s : s + 1]
            mem[s, h] = decay[s : s + 1, h : h + 1] * mem[s, h] + column * value[s : s + 1, h * DV : (h + 1) * DV]
    put = pltpu.make_async_copy(mem, newmem_h, local_sem.at[14])
    put.start()
    finish()

    partial = lax.dot_general(wmix_t[...], gated[...], (((1,), (1,)), ((), ())), preferred_element_type=F32)
    total = sum_over_tp(partial, mix_send, mix_recv, (m_s, m_r))
    mixed = (token_t[rows(tp, mine), :].astype(F32) + total).astype(BF16)
    mixed_t[rows(tp, mine), :] = mixed
    for d in far_first(n_tp):
        part = mixed_t.at[rows(tp, mine), :]
        send(part, part, x_s.at[d], x_r.at[d], {"tp": tp_of(d)})
    loads["gate"].wait()
    loads["up"].wait()
    for d in near_first(n_tp):
        arrive(mixed_t.at[rows(from_tp(d), mine), :], x_s.at[d], x_r.at[d], {"tp": tp_of(d)})

    u_total = z2_own.at[y]
    x_raw[...] = mixed_t[...].T.reshape(x_raw.shape)
    reduce_over_kv(
        ffn_gain, w2, 2 * n_ff, 0, False, z2_pair, z2_own, z2_got, z2_send, z2_recv, (p2_s, p2_r, b_s, b_r), u_total
    )
    squares = tile_of(u_total, z2_recv, 2 * n_ff)[:, :1]
    scale2 = lax.rsqrt(squares / n_feats + 1e-06)
    for at, size in column_pieces(n_ff):
        gate = scale2 * total_of(u_total, z2_recv, at, size)
        up = scale2 * total_of(u_total, z2_recv, n_ff + at, size)
        hidden[rows(kv, own), at : at + size] = (gate * jax.nn.sigmoid(gate) * up).astype(BF16)
    gather_over_kv(hidden, (h_s, h_r, hf_s, hf_r))()

    partial = lax.dot_general(wd_t[...], hidden[...], (((1,), (1,)), ((), ())), preferred_element_type=F32)
    total = sum_over_tp(partial, down_send, down_recv, (d_s, d_r))
    out_ref[...] = (mixed_t[rows(tp, mine), :].astype(F32) + total).astype(BF16)
    put.wait()
    for copy in sent:
        copy.wait_send()


def shards(n_kv, n_tp, tokens, norm_gain, w_query, w_key, w_value, w_outgate, w_input_gate, w_forget_gate, memory, normalizer, stabilizer, w_mix_out, ffn_gain, w_gate, w_up, w_down):
    seqs, mine = tokens.shape
    feats = norm_gain.shape[0]
    n_y = n_kv // 2
    own = memory.shape[0]
    dv = w_value.shape[1]
    n1 = w_query.shape[1] + w_key.shape[1] + 2 * dv + LANES
    n_ff = w_gate.shape[1]
    n2 = 2 * n_ff + LANES
    out_feats = w_mix_out.shape[1]
    hbm = pl.BlockSpec(memory_space=pltpu.HBM)
    vmem = pl.BlockSpec(memory_space=pltpu.VMEM)
    dma = pltpu.SemaphoreType.DMA
    ys, xs, one = dma((n_y,)), dma((n_tp,)), dma
    out_t, new_memory, new_normalizer, new_stabilizer = pl.pallas_call(
        functools.partial(layer_kernel, n_kv, n_tp),
        out_shape=(
            jax.ShapeDtypeStruct((mine, seqs), BF16),
            jax.ShapeDtypeStruct(memory.shape, F32),
            jax.ShapeDtypeStruct(normalizer.shape, F32),
            jax.ShapeDtypeStruct(stabilizer.shape, F32),
        ),
        in_specs=[hbm, vmem] + [hbm] * 10 + [vmem] + [hbm] * 3,
        out_specs=(vmem, hbm, vmem, vmem),
        scratch_shapes=[
            pltpu.VMEM(tokens.shape, BF16),
            pltpu.VMEM((feats, n1), BF16),
            pltpu.VMEM((2, *w_input_gate.shape), BF16),
            pltpu.VMEM(memory.shape, F32),
            pltpu.VMEM(normalizer.shape, F32),
            pltpu.VMEM(stabilizer.shape, F32),
            pltpu.VMEM(w_mix_out.shape, BF16),
            pltpu.VMEM(w_mix_out.shape[::-1], BF16),
            pltpu.VMEM((feats, 2 * n_ff), BF16),
            pltpu.VMEM(w_down.shape, BF16),
            pltpu.VMEM(w_down.shape[::-1], BF16),
            pltpu.VMEM((feats, seqs), BF16),
            pltpu.VMEM((n_y, 2, own, feats), BF16),
            pltpu.VMEM((n_y, own, n1), BF16),
            pltpu.VMEM((n_y, own, n1), F32),
            pltpu.VMEM((n_y, own, n1), BF16),
            pltpu.VMEM((n_y, own, n1), BF16),
            pltpu.VMEM((n_y, own, n1), BF16),
            pltpu.VMEM((own, dv), F32),
            pltpu.VMEM((seqs, dv), BF16),
            pltpu.VMEM((n_tp, mine, seqs), BF16),
            pltpu.VMEM((n_tp, mine, seqs), BF16),
            pltpu.VMEM((out_feats, seqs), BF16),
            pltpu.VMEM((n_y, own, n2), BF16),
            pltpu.VMEM((n_y, own, n2), F32),
            pltpu.VMEM((n_y, own, n2), BF16),
            pltpu.VMEM((n_y, own, n2), BF16),
            pltpu.VMEM((n_y, own, n2), BF16),
            pltpu.VMEM((seqs, n_ff), BF16),
            pltpu.VMEM((n_tp, mine, seqs), BF16),
            pltpu.VMEM((n_tp, mine, seqs), BF16),
            dma((15,)),
            xs, xs,
            one, one, ys, ys,
            ys, ys, ys, ys,
            xs, xs,
            xs, xs,
            one, one, ys, ys,
            ys, ys, ys, ys,
            xs, xs,
        ],
        compiler_params=pltpu.CompilerParams(collective_id=0, has_side_effects=True, vmem_limit_bytes=48 * 1024 * 1024),
        name="layer",
    )(
        tokens, norm_gain.reshape(1, -1), w_query, w_key, w_value, w_outgate, w_input_gate, w_forget_gate,
        memory, normalizer, stabilizer, w_mix_out, ffn_gain.reshape(1, -1), w_gate, w_up, w_down,
    )
    return out_t.T, new_memory, new_normalizer, new_stabilizer


def solution(mesh):
    in_specs = (
        P("grp", ("kv", "tp")),
        P("kv"),
        P("kv", "tp"),
        P("kv", "tp"),
        P("kv", "tp"),
        P("kv", "tp"),
        P("kv", None),
        P("kv", None),
        P(("grp", "kv"), "tp", None, None),
        P(("grp", "kv"), "tp", None),
        P(("grp", "kv"), "tp"),
        P("tp", "kv"),
        P("kv"),
        P("kv", "tp"),
        P("kv", "tp"),
        P("tp", "kv"),
    )
    out_specs = (
        P("grp", ("kv", "tp")),
        P(("grp", "kv"), "tp", None, None),
        P(("grp", "kv"), "tp", None),
        P(("grp", "kv"), "tp"),
    )
    body = functools.partial(shards, mesh.shape["kv"], mesh.shape["tp"])
    return jax.shard_map(body, mesh=mesh, in_specs=in_specs, out_specs=out_specs, check_vma=False)
```

```python
import functools

import jax
import jax.numpy as jnp
from jax import lax
from jax.experimental import pallas as pl
from jax.experimental.pallas import tpu as pltpu
from jax.sharding import PartitionSpec as P

DQK = 64
DV = 128
LANES = 128
HALF = LANES // 2
F32 = jnp.float32
BF16 = jnp.bfloat16
MESH = pl.DeviceIdType.MESH


def far_first(count):
    return sorted(range(1, count), key=lambda d: -min(d, count - d))


def near_first(count):
    return far_first(count)[::-1]


def column_pieces(width, step=256):
    return [(at, min(step, width - at)) for at in range(0, width, step)]


def hi_lo(values, lane):
    high = values.astype(BF16).astype(F32)
    return jnp.where(lane < HALF, high, values - high).astype(BF16)


def from_hi_lo(tile):
    return tile[:, :HALF] + tile[:, HALF:]


def layer_kernel(
    n_kv, n_tp,
    tokens_h, norm_gain, wq_h, wk_h, wv_h, wo_h, wi_h, wf_h, mem_h, norm_h, stab_h, wmix_h, ffn_gain, wg_h, wu_h, wd_h,
    out_ref, newmem_h, newnorm_ref, newstab_ref,
    w1, wgates, mem, norm, stab, wmix, wmix_t, w2, wd, wd_t,
    token_t, x_raw, z1_pair, z1_own, z1_got, z1_send, z1_recv,
    numer, gated, mix_send, mix_recv, mixed_t, z2_pair, z2_own, z2_got, z2_send, z2_recv, hidden, down_send, down_recv,
    local_sem, tok_s, tok_r, p1_s, p1_r, a_s, a_r, g_s, g_r, gf_s, gf_r, m_s, m_r, x_s, x_r, p2_s, p2_r, b_s, b_r, h_s, h_r, hf_s, hf_r, d_s, d_r,
):
    kv, tp = lax.axis_index("kv"), lax.axis_index("tp")
    n_y = n_kv // 2
    core, y = lax.rem(kv, 2), kv // 2
    other = 1 - core
    partner = 2 * y + other
    own = mem.shape[0]
    heads = mem.shape[1]
    feats = token_t.shape[0]
    mine = tokens_h.shape[0]
    half_rows = n_y * own
    n_feats = feats * n_kv

    def y_of(d):
        return lax.rem(y + d, n_y)

    def from_y(d):
        return lax.rem(y + n_y - d, n_y)

    def tp_of(d):
        return lax.rem(tp + d, n_tp)

    def from_tp(d):
        return lax.rem(tp + n_tp - d, n_tp)

    def rows(index, size):
        return pl.ds(pl.multiple_of(index * size, size), size)

    barrier = pltpu.get_barrier_semaphore()
    for d in far_first(n_tp):
        pl.semaphore_signal(barrier, inc=1, device_id={"tp": tp_of(d)}, device_id_type=MESH)
    for d in far_first(n_y):
        pl.semaphore_signal(barrier, inc=1, device_id={"kv": 2 * y_of(d) + core}, device_id_type=MESH)
    pl.semaphore_signal(barrier, inc=1, device_id={"kv": partner}, device_id_type=MESH)

    dq, dk, dv = wq_h.shape[1], wk_h.shape[1], wv_h.shape[1]
    n_main = dq + dk + 2 * dv
    n_ff = wg_h.shape[1]
    n_gate = wi_h.shape[0]
    loads = {}
    for i, (name, source, target) in enumerate((
        ("tokens", tokens_h, token_t.at[rows(tp, mine), :]),
        ("wi", wi_h, wgates.at[pl.ds(0, n_gate), :]),
        ("wf", wf_h, wgates.at[pl.ds(n_gate, n_gate), :]),
        ("wq", wq_h, w1.at[:, pl.ds(0, dq)]),
        ("wk", wk_h, w1.at[:, pl.ds(dq, dk)]),
        ("wv", wv_h, w1.at[:, pl.ds(dq + dk, dv)]),
        ("wo", wo_h, w1.at[:, pl.ds(dq + dk + dv, dv)]),
        ("mix", wmix_h, wmix),
        ("down", wd_h, wd),
        ("mem", mem_h, mem),
        ("norm", norm_h, norm),
        ("stab", stab_h, stab),
        ("gate", wg_h, w2.at[:, pl.ds(0, n_ff)]),
        ("up", wu_h, w2.at[:, pl.ds(n_ff, n_ff)]),
    )):
        loads[name] = pltpu.make_async_copy(source, target, local_sem.at[i])
        loads[name].start()
    sent = []

    def send(source, target, send_sem, recv_sem, where):
        copy = pltpu.make_async_remote_copy(
            src_ref=source, dst_ref=target, send_sem=send_sem, recv_sem=recv_sem, device_id=where, device_id_type=MESH
        )
        copy.start()
        sent.append(copy)

    def arrive(target, send_sem, recv_sem, where):
        pltpu.make_async_remote_copy(
            src_ref=target, dst_ref=target, send_sem=send_sem, recv_sem=recv_sem, device_id=where, device_id_type=MESH
        ).wait_recv()

    loads["tokens"].wait()
    pl.semaphore_wait(barrier, (n_tp - 1) + (n_y - 1) + 1)
    for d in far_first(n_tp):
        part = token_t.at[rows(tp, mine), :]
        send(part, part, tok_s.at[d], tok_r.at[d], {"tp": tp_of(d)})

    loads["wi"].wait()
    loads["wf"].wait()
    lane_w = lax.rem(lax.broadcasted_iota(jnp.int32, (2 * n_gate, LANES), 1), HALF)
    row_w = lax.broadcasted_iota(jnp.int32, (2 * n_gate, LANES), 0)
    is_f = row_w // n_gate
    head = row_w - is_f * n_gate - tp * heads
    pick = jnp.where((head >= 0) & (head < heads) & (lane_w == head + heads * is_f), 1.0, 0.0).astype(BF16)
    w1[:, n_main:] = lax.dot_general(
        wgates[...], pick, (((0,), (0,)), ((), ())), preferred_element_type=F32
    ).astype(BF16)

    loads["mix"].wait()
    wmix_t[...] = wmix[...].T
    loads["down"].wait()
    for at, width in column_pieces(wd.shape[0]):
        wd_t[:, at : at + width] = wd[at : at + width, :].T
    for name in ("wq", "wk", "wv", "wo"):
        loads[name].wait()

    for d in near_first(n_tp):
        arrive(token_t.at[rows(from_tp(d), mine), :], tok_s.at[d], tok_r.at[d], {"tp": tp_of(d)})

    lane = lax.broadcasted_iota(jnp.int32, (half_rows, LANES), 1)

    def project(gain, weights, widths, square_lane, gates, core_of, store):
        wide = x_raw[:, core_of].reshape(half_rows, feats).astype(F32)
        normed = (wide * gain[...].astype(F32)[None, :]).astype(BF16)
        squares = jnp.sum(wide * wide, axis=1, keepdims=True)
        for at, width in widths:
            store(at, width, jnp.dot(normed, weights[:, at : at + width], preferred_element_type=F32))
        end = widths[-1][0] + widths[-1][1]
        tile = jnp.broadcast_to(squares, (half_rows, LANES))
        if gates:
            last = jnp.dot(normed, weights[:, end : end + LANES], preferred_element_type=F32)
            tile = jnp.where(lax.rem(lane, HALF) == square_lane, tile, last)
        store(end, LANES, tile)

    def reduce_over_kv(gain, weights, width, square_lane, gates, pair, own_z, got, out, into, sems, total_at):
        p_s, p_r, r_s, r_r = sems
        pieces = column_pieces(width)

        def to_partner(at, size, z):
            value = hi_lo(z, lane) if at == width else z.astype(BF16)
            pair[:, :, at : at + size] = value.reshape(n_y, own, size)

        def keep(at, size, z):
            own_z[:, :, at : at + size] = z.reshape(n_y, own, size)

        project(gain, weights, pieces, square_lane, gates, other, to_partner)
        send(pair, got, p_s, p_r, {"kv": partner})
        project(gain, weights, pieces, square_lane, gates, core, keep)
        arrive(got, p_s, p_r, {"kv": partner})
        small_lane = lax.broadcasted_iota(jnp.int32, (own, LANES), 1)
        for d in far_first(n_y) + [0]:
            at_y = y_of(d)
            for at, size in pieces + [(width, LANES)]:
                both = own_z[at_y, :, at : at + size]
                other_half = got[at_y, :, at : at + size].astype(F32)
                if at == width:
                    both = both + (other_half + jnp.concatenate([other_half[:, HALF:], other_half[:, :HALF]], axis=1))
                    if d:
                        both = hi_lo(both, small_lane)
                else:
                    both = both + other_half
                if d:
                    out[d, :, at : at + size] = both.astype(BF16)
                else:
                    total_at[:, at : at + size] = both
            if d:
                send(out.at[d], into.at[d], r_s.at[d], r_r.at[d], {"kv": 2 * at_y + core})
        for d in near_first(n_y):
            arrive(into.at[d], r_s.at[d], r_r.at[d], {"kv": 2 * y_of(d) + core})

    def total_of(total_at, into, at, size):
        value = total_at[:, at : at + size]
        for d in range(1, n_y):
            value = value + into[d, :, at : at + size].astype(F32)
        return value

    def tile_of(total_at, into, at):
        rest = into[1, :, at : at + LANES].astype(F32)
        for d in range(2, n_y):
            rest = rest + into[d, :, at : at + LANES].astype(F32)
        return total_at[:, at : at + HALF] + from_hi_lo(rest)

    def gather_over_kv(buffer, sems):
        r_s, r_r, f_s, f_r = sems
        part = buffer.at[rows(kv, own), :]
        for d in far_first(n_y):
            send(part, part, r_s.at[d], r_r.at[d], {"kv": 2 * y_of(d) + core})
        send(part, part, f_s.at[0], f_r.at[0], {"kv": partner})

        def finish():
            for d in near_first(n_y):
                got = buffer.at[rows(2 * from_y(d) + core, own), :]
                arrive(got, r_s.at[d], r_r.at[d], {"kv": 2 * y_of(d) + core})
                send(got, got, f_s.at[d], f_r.at[d], {"kv": partner})
            for d in [0] + near_first(n_y):
                arrive(buffer.at[rows(2 * from_y(d) + other, own), :], f_s.at[d], f_r.at[d], {"kv": partner})

        return finish

    def sum_over_tp(partial, out, into, sems):
        s, r = sems
        out[...] = partial.astype(BF16).reshape(n_tp, mine, partial.shape[1])
        for d in far_first(n_tp):
            send(out.at[tp_of(d)], into.at[d], s.at[d], r.at[d], {"tp": tp_of(d)})
        total = out[tp].astype(F32)
        for d in near_first(n_tp):
            arrive(into.at[d], s.at[d], r.at[d], {"tp": tp_of(d)})
            total = total + into[d].astype(F32)
        return total

    z_total = z1_own.at[y]
    x_raw[...] = token_t[...].T.reshape(x_raw.shape)
    reduce_over_kv(
        norm_gain, w1, n_main, 2 * heads, True, z1_pair, z1_own, z1_got, z1_send, z1_recv, (p1_s, p1_r, a_s, a_r), z_total
    )
    gates = tile_of(z_total, z1_recv, n_main)
    scale1 = lax.rsqrt(gates[:, 2 * heads : 2 * heads + 1] / n_feats + 1e-06)
    query = scale1 * total_of(z_total, z1_recv, 0, dq) * DQK ** (-0.5)
    key = scale1 * total_of(z_total, z1_recv, dq, dk)
    value = scale1 * total_of(z_total, z1_recv, dq + dk, dv)
    outgate = scale1 * total_of(z_total, z1_recv, dq + dk + dv, dv)
    igate = scale1 * gates[:, :heads]
    forget = scale1 * gates[:, heads : 2 * heads]
    lforget = jnp.minimum(forget, 0.0) - jnp.log1p(jnp.exp(-jnp.abs(forget)))
    loads["stab"].wait()
    loads["norm"].wait()
    loads["mem"].wait()
    held = lforget + stab[...].T
    new_stab = jnp.maximum(held, igate)
    newstab_ref[...] = new_stab.T
    decay = jnp.exp(held - new_stab)
    inflow = jnp.exp(igate - new_stab)
    floor = jnp.exp(-new_stab)
    query_t = query.T
    for s in range(own):
        for h in range(heads):
            column = query_t[h * DQK : (h + 1) * DQK, s : s + 1]
            numer[s : s + 1, h * DV : (h + 1) * DV] = jnp.sum(column * mem[s, h], axis=0, keepdims=True)
    for h in range(heads):
        q, k = query[:, h * DQK : (h + 1) * DQK], key[:, h * DQK : (h + 1) * DQK]
        keep, add = decay[:, h : h + 1], inflow[:, h : h + 1]
        new_norm = keep * norm[:, h, :] + add * k
        newnorm_ref[:, h, :] = new_norm
        denom = jnp.maximum(jnp.abs(jnp.sum(q * new_norm, axis=1, keepdims=True)), floor[:, h : h + 1])
        at = slice(h * DV, (h + 1) * DV)
        top = keep * numer[:, at] + (add * jnp.sum(q * k, axis=1, keepdims=True)) * value[:, at]
        gated[rows(kv, own), at] = (jax.nn.sigmoid(outgate[:, at]) * (top / denom)).astype(BF16)
    finish = gather_over_kv(gated, (g_s, g_r, gf_s, gf_r))

    spread = jnp.concatenate([jnp.broadcast_to(inflow[:, h : h + 1], (own, DQK)) for h in range(heads)], axis=1)
    key_t = (key * spread).T
    for s in range(own):
        for h in range(heads):
            column = key_t[h * DQK : (h + 1) * DQK, s : s + 1]
            mem[s, h] = decay[s : s + 1, h : h + 1] * mem[s, h] + column * value[s : s + 1, h * DV : (h + 1) * DV]
    put = pltpu.make_async_copy(mem, newmem_h, local_sem.at[14])
    put.start()
    finish()

    partial = lax.dot_general(wmix_t[...], gated[...], (((1,), (1,)), ((), ())), preferred_element_type=F32)
    total = sum_over_tp(partial, mix_send, mix_recv, (m_s, m_r))
    mixed = (token_t[rows(tp, mine), :].astype(F32) + total).astype(BF16)
    mixed_t[rows(tp, mine), :] = mixed
    for d in far_first(n_tp):
        part = mixed_t.at[rows(tp, mine), :]
        send(part, part, x_s.at[d], x_r.at[d], {"tp": tp_of(d)})
    loads["gate"].wait()
    loads["up"].wait()
    for d in near_first(n_tp):
        arrive(mixed_t.at[rows(from_tp(d), mine), :], x_s.at[d], x_r.at[d], {"tp": tp_of(d)})

    u_total = z2_own.at[y]
    x_raw[...] = mixed_t[...].T.reshape(x_raw.shape)
    reduce_over_kv(
        ffn_gain, w2, 2 * n_ff, 0, False, z2_pair, z2_own, z2_got, z2_send, z2_recv, (p2_s, p2_r, b_s, b_r), u_total
    )
    squares = tile_of(u_total, z2_recv, 2 * n_ff)[:, :1]
    scale2 = lax.rsqrt(squares / n_feats + 1e-06)
    for at, size in column_pieces(n_ff):
        gate = scale2 * total_of(u_total, z2_recv, at, size)
        up = scale2 * total_of(u_total, z2_recv, n_ff + at, size)
        hidden[rows(kv, own), at : at + size] = (gate * jax.nn.sigmoid(gate) * up).astype(BF16)
    gather_over_kv(hidden, (h_s, h_r, hf_s, hf_r))()

    partial = lax.dot_general(wd_t[...], hidden[...], (((1,), (1,)), ((), ())), preferred_element_type=F32)
    total = sum_over_tp(partial, down_send, down_recv, (d_s, d_r))
    out_ref[...] = (mixed_t[rows(tp, mine), :].astype(F32) + total).astype(BF16)
    put.wait()
    for copy in sent:
        copy.wait_send()


def shards(n_kv, n_tp, tokens, norm_gain, w_query, w_key, w_value, w_outgate, w_input_gate, w_forget_gate, memory, normalizer, stabilizer, w_mix_out, ffn_gain, w_gate, w_up, w_down):
    seqs, mine = tokens.shape
    feats = norm_gain.shape[0]
    n_y = n_kv // 2
    own = memory.shape[0]
    dv = w_value.shape[1]
    n1 = w_query.shape[1] + w_key.shape[1] + 2 * dv + LANES
    n_ff = w_gate.shape[1]
    n2 = 2 * n_ff + LANES
    out_feats = w_mix_out.shape[1]
    hbm = pl.BlockSpec(memory_space=pltpu.HBM)
    vmem = pl.BlockSpec(memory_space=pltpu.VMEM)
    dma = pltpu.SemaphoreType.DMA
    ys, xs, one = dma((n_y,)), dma((n_tp,)), dma
    out_t, new_memory, new_normalizer, new_stabilizer = pl.pallas_call(
        functools.partial(layer_kernel, n_kv, n_tp),
        out_shape=(
            jax.ShapeDtypeStruct((mine, seqs), BF16),
            jax.ShapeDtypeStruct(memory.shape, F32),
            jax.ShapeDtypeStruct(normalizer.shape, F32),
            jax.ShapeDtypeStruct(stabilizer.shape[::-1], F32),
        ),
        in_specs=[hbm, vmem] + [hbm] * 10 + [vmem] + [hbm] * 3,
        out_specs=(vmem, hbm, vmem, vmem),
        scratch_shapes=[
            pltpu.VMEM((feats, n1), BF16),
            pltpu.VMEM((2 * w_input_gate.shape[1], feats), BF16),
            pltpu.VMEM(memory.shape, F32),
            pltpu.VMEM(normalizer.shape, F32),
            pltpu.VMEM(stabilizer.shape[::-1], F32),
            pltpu.VMEM(w_mix_out.shape, BF16),
            pltpu.VMEM(w_mix_out.shape[::-1], BF16),
            pltpu.VMEM((feats, 2 * n_ff), BF16),
            pltpu.VMEM(w_down.shape, BF16),
            pltpu.VMEM(w_down.shape[::-1], BF16),
            pltpu.VMEM((feats, seqs), BF16),
            pltpu.VMEM((n_y, 2, own, feats), BF16),
            pltpu.VMEM((n_y, own, n1), BF16),
            pltpu.VMEM((n_y, own, n1), F32),
            pltpu.VMEM((n_y, own, n1), BF16),
            pltpu.VMEM((n_y, own, n1), BF16),
            pltpu.VMEM((n_y, own, n1), BF16),
            pltpu.VMEM((own, dv), F32),
            pltpu.VMEM((seqs, dv), BF16),
            pltpu.VMEM((n_tp, mine, seqs), BF16),
            pltpu.VMEM((n_tp, mine, seqs), BF16),
            pltpu.VMEM((out_feats, seqs), BF16),
            pltpu.VMEM((n_y, own, n2), BF16),
            pltpu.VMEM((n_y, own, n2), F32),
            pltpu.VMEM((n_y, own, n2), BF16),
            pltpu.VMEM((n_y, own, n2), BF16),
            pltpu.VMEM((n_y, own, n2), BF16),
            pltpu.VMEM((seqs, n_ff), BF16),
            pltpu.VMEM((n_tp, mine, seqs), BF16),
            pltpu.VMEM((n_tp, mine, seqs), BF16),
            dma((15,)),
            xs, xs,
            one, one, ys, ys,
            ys, ys, ys, ys,
            xs, xs,
            xs, xs,
            one, one, ys, ys,
            ys, ys, ys, ys,
            xs, xs,
        ],
        compiler_params=pltpu.CompilerParams(collective_id=0, has_side_effects=True, vmem_limit_bytes=67_043_328),
        name="layer",
    )(
        tokens.T, norm_gain, w_query, w_key, w_value, w_outgate, w_input_gate.T, w_forget_gate.T,
        memory, normalizer, stabilizer.T, w_mix_out, ffn_gain, w_gate, w_up, w_down,
    )
    return out_t.T, new_memory, new_normalizer, new_stabilizer.T


def solution(mesh):
    in_specs = (
        P("grp", ("kv", "tp")),
        P("kv"),
        P("kv", "tp"),
        P("kv", "tp"),
        P("kv", "tp"),
        P("kv", "tp"),
        P("kv", None),
        P("kv", None),
        P(("grp", "kv"), "tp", None, None),
        P(("grp", "kv"), "tp", None),
        P(("grp", "kv"), "tp"),
        P("tp", "kv"),
        P("kv"),
        P("kv", "tp"),
        P("kv", "tp"),
        P("tp", "kv"),
    )
    out_specs = (
        P("grp", ("kv", "tp")),
        P(("grp", "kv"), "tp", None, None),
        P(("grp", "kv"), "tp", None),
        P(("grp", "kv"), "tp"),
    )
    body = functools.partial(shards, mesh.shape["kv"], mesh.shape["tp"])
    return jax.shard_map(body, mesh=mesh, in_specs=in_specs, out_specs=out_specs, check_vma=False)
```

```python
import functools

import jax
import jax.numpy as jnp
from jax import lax
from jax.experimental import pallas as pl
from jax.experimental.pallas import tpu as pltpu
from jax.sharding import PartitionSpec as P

DQK = 64
DV = 128
LANES = 128
HALF = LANES // 2
FF_CHUNK = 3 * LANES
F32 = jnp.float32
BF16 = jnp.bfloat16
MESH = pl.DeviceIdType.MESH


def far_first(count):
    return sorted(range(1, count), key=lambda d: -min(d, count - d))


def near_first(count):
    return far_first(count)[::-1]


def column_pieces(width, step=256):
    return [(at, min(step, width - at)) for at in range(0, width, step)]


def ff_chunks(width):
    return column_pieces(width, FF_CHUNK)


def hi_lo(values, lane):
    high = values.astype(BF16).astype(F32)
    return jnp.where(lane < HALF, high, values - high).astype(BF16)


def from_hi_lo(tile):
    return tile[:, :HALF] + tile[:, HALF:]


def layer_kernel(
    n_kv, n_tp,
    tokens_h, norm_gain, wq_h, wk_h, wv_h, wo_h, wi_h, wf_h, mem_h, norm_h, stab_h, wmix_h, ffn_gain, wg_h, wu_h, wd_h,
    out_ref, newmem_h, newnorm_ref, newstab_ref,
    w1, wgates, mem, norm, stab, wmix, wmix_t, w2, wd, wd_t,
    token_t, x_raw, z1_pair, z1_own, z1_got, z1_send, z1_recv,
    numer, gated, mix_send, mix_recv, mixed_t, z2_pair, z2_own, z2_got, z2_send, z2_recv, hidden, down_sum, down_send, down_recv,
    local_sem, tok_s, tok_r, p1_s, p1_r, a_s, a_r, g_s, g_r, gf_s, gf_r, m_s, m_r, x_s, x_r, p2_s, p2_r, b_s, b_r, h_s, h_r, hf_s, hf_r, d_s, d_r,
):
    kv, tp = lax.axis_index("kv"), lax.axis_index("tp")
    n_y = n_kv // 2
    core, y = lax.rem(kv, 2), kv // 2
    other = 1 - core
    partner = 2 * y + other
    own = mem.shape[0]
    heads = mem.shape[1]
    feats = token_t.shape[0]
    mine = tokens_h.shape[0]
    half_rows = n_y * own
    n_feats = feats * n_kv

    def y_of(d):
        return lax.rem(y + d, n_y)

    def from_y(d):
        return lax.rem(y + n_y - d, n_y)

    def tp_of(d):
        return lax.rem(tp + d, n_tp)

    def from_tp(d):
        return lax.rem(tp + n_tp - d, n_tp)

    def rows(index, size):
        return pl.ds(pl.multiple_of(index * size, size), size)

    barrier = pltpu.get_barrier_semaphore()
    for d in far_first(n_tp):
        pl.semaphore_signal(barrier, inc=1, device_id={"tp": tp_of(d)}, device_id_type=MESH)
    for d in far_first(n_y):
        pl.semaphore_signal(barrier, inc=1, device_id={"kv": 2 * y_of(d) + core}, device_id_type=MESH)
    pl.semaphore_signal(barrier, inc=1, device_id={"kv": partner}, device_id_type=MESH)

    dq, dk, dv = wq_h.shape[1], wk_h.shape[1], wv_h.shape[1]
    n_main = dq + dk + 2 * dv
    n_ff = wg_h.shape[1]
    n_gate = wi_h.shape[0]
    loads = {}
    for i, (name, source, target) in enumerate((
        ("tokens", tokens_h, token_t.at[rows(tp, mine), :]),
        ("wi", wi_h, wgates.at[pl.ds(0, n_gate), :]),
        ("wf", wf_h, wgates.at[pl.ds(n_gate, n_gate), :]),
        ("wq", wq_h, w1.at[:, pl.ds(0, dq)]),
        ("wk", wk_h, w1.at[:, pl.ds(dq, dk)]),
        ("wv", wv_h, w1.at[:, pl.ds(dq + dk, dv)]),
        ("wo", wo_h, w1.at[:, pl.ds(dq + dk + dv, dv)]),
        ("mix", wmix_h, wmix),
        ("down", wd_h, wd),
        ("mem", mem_h, mem),
        ("norm", norm_h, norm),
        ("stab", stab_h, stab),
    ) + tuple(
        (f"{name}{at}", source.at[:, pl.ds(at, size)], w2.at[:, pl.ds(2 * at + shift * size, size)])
        for at, size in ff_chunks(n_ff)
        for shift, (name, source) in enumerate((("gate", wg_h), ("up", wu_h)))
    )):
        loads[name] = pltpu.make_async_copy(source, target, local_sem.at[i + (i >= 12)])
        loads[name].start()
    sent = []

    def send(source, target, send_sem, recv_sem, where):
        copy = pltpu.make_async_remote_copy(
            src_ref=source, dst_ref=target, send_sem=send_sem, recv_sem=recv_sem, device_id=where, device_id_type=MESH
        )
        copy.start()
        sent.append(copy)

    def arrive(target, send_sem, recv_sem, where):
        pltpu.make_async_remote_copy(
            src_ref=target, dst_ref=target, send_sem=send_sem, recv_sem=recv_sem, device_id=where, device_id_type=MESH
        ).wait_recv()

    loads["tokens"].wait()
    with jax.named_scope("barrier"):
        pl.semaphore_wait(barrier, (n_tp - 1) + (n_y - 1) + 1)
    for d in far_first(n_tp):
        part = token_t.at[rows(tp, mine), :]
        send(part, part, tok_s.at[d], tok_r.at[d], {"tp": tp_of(d)})

    loads["wi"].wait()
    loads["wf"].wait()
    with jax.named_scope("prep"):
        lane_w = lax.rem(lax.broadcasted_iota(jnp.int32, (2 * n_gate, LANES), 1), HALF)
        row_w = lax.broadcasted_iota(jnp.int32, (2 * n_gate, LANES), 0)
        is_f = row_w // n_gate
        head = row_w - is_f * n_gate - tp * heads
        pick = jnp.where((head >= 0) & (head < heads) & (lane_w == head + heads * is_f), 1.0, 0.0).astype(BF16)
        w1[:, n_main:] = lax.dot_general(
            wgates[...], pick, (((0,), (0,)), ((), ())), preferred_element_type=F32
        ).astype(BF16)

        loads["mix"].wait()
        wmix_t[...] = wmix[...].T
        loads["down"].wait()
        for at, width in column_pieces(wd.shape[0]):
            wd_t[:, at : at + width] = wd[at : at + width, :].T
        for name in ("wq", "wk", "wv", "wo"):
            loads[name].wait()

    with jax.named_scope("wait_tok"):
        for d in near_first(n_tp):
            arrive(token_t.at[rows(from_tp(d), mine), :], tok_s.at[d], tok_r.at[d], {"tp": tp_of(d)})

    lane = lax.broadcasted_iota(jnp.int32, (half_rows, LANES), 1)

    def project(gain, weights, widths, square_lane, gates, core_of, store):
        wide = x_raw[:, core_of].reshape(half_rows, feats).astype(F32)
        normed = (wide * gain[...].astype(F32)[None, :]).astype(BF16)
        squares = jnp.sum(wide * wide, axis=1, keepdims=True)
        for at, width in widths:
            store(at, width, jnp.dot(normed, weights[:, at : at + width], preferred_element_type=F32))
        end = widths[-1][0] + widths[-1][1]
        tile = jnp.broadcast_to(squares, (half_rows, LANES))
        if gates:
            last = jnp.dot(normed, weights[:, end : end + LANES], preferred_element_type=F32)
            tile = jnp.where(lax.rem(lane, HALF) == square_lane, tile, last)
        store(end, LANES, tile)

    def reduce_over_kv(gain, weights, width, square_lane, gates, pair, own_z, got, out, into, sems, total_at):
        p_s, p_r, r_s, r_r = sems
        pieces = column_pieces(width)

        def to_partner(at, size, z):
            value = hi_lo(z, lane) if at == width else z.astype(BF16)
            pair[:, :, at : at + size] = value.reshape(n_y, own, size)

        def keep(at, size, z):
            own_z[:, :, at : at + size] = z.reshape(n_y, own, size)

        with jax.named_scope("proj"):
            project(gain, weights, pieces, square_lane, gates, other, to_partner)
            send(pair, got, p_s, p_r, {"kv": partner})
            project(gain, weights, pieces, square_lane, gates, core, keep)
        with jax.named_scope("wait_pair"):
            arrive(got, p_s, p_r, {"kv": partner})
        small_lane = lax.broadcasted_iota(jnp.int32, (own, LANES), 1)
        with jax.named_scope("pairsum"):
            for d in far_first(n_y) + [0]:
                at_y = y_of(d)
                for at, size in pieces + [(width, LANES)]:
                    both = own_z[at_y, :, at : at + size]
                    other_half = got[at_y, :, at : at + size].astype(F32)
                    if at == width:
                        both = both + (other_half + jnp.concatenate([other_half[:, HALF:], other_half[:, :HALF]], axis=1))
                        if d:
                            both = hi_lo(both, small_lane)
                    else:
                        both = both + other_half
                    if d:
                        out[d, :, at : at + size] = both.astype(BF16)
                    else:
                        total_at[:, at : at + size] = both
                if d:
                    send(out.at[d], into.at[d], r_s.at[d], r_r.at[d], {"kv": 2 * at_y + core})
        with jax.named_scope("wait_rs"):
            for d in near_first(n_y):
                arrive(into.at[d], r_s.at[d], r_r.at[d], {"kv": 2 * y_of(d) + core})

    def total_of(total_at, into, at, size):
        value = total_at[:, at : at + size]
        for d in range(1, n_y):
            value = value + into[d, :, at : at + size].astype(F32)
        return value

    def tile_of(total_at, into, at):
        rest = into[1, :, at : at + LANES].astype(F32)
        for d in range(2, n_y):
            rest = rest + into[d, :, at : at + LANES].astype(F32)
        return total_at[:, at : at + HALF] + from_hi_lo(rest)

    def gather_over_kv(buffer, sems):
        r_s, r_r, f_s, f_r = sems
        part = buffer.at[rows(kv, own), :]
        for d in far_first(n_y):
            send(part, part, r_s.at[d], r_r.at[d], {"kv": 2 * y_of(d) + core})
        send(part, part, f_s.at[0], f_r.at[0], {"kv": partner})

        def finish():
            for d in near_first(n_y):
                got = buffer.at[rows(2 * from_y(d) + core, own), :]
                arrive(got, r_s.at[d], r_r.at[d], {"kv": 2 * y_of(d) + core})
                send(got, got, f_s.at[d], f_r.at[d], {"kv": partner})
            for d in [0] + near_first(n_y):
                arrive(buffer.at[rows(2 * from_y(d) + other, own), :], f_s.at[d], f_r.at[d], {"kv": partner})

        return finish

    def sum_over_tp(partial, out, into, sems):
        s, r = sems
        out[...] = partial.astype(BF16).reshape(n_tp, mine, partial.shape[1])
        for d in far_first(n_tp):
            send(out.at[tp_of(d)], into.at[d], s.at[d], r.at[d], {"tp": tp_of(d)})
        total = out[tp].astype(F32)
        for d in near_first(n_tp):
            arrive(into.at[d], s.at[d], r.at[d], {"tp": tp_of(d)})
            total = total + into[d].astype(F32)
        return total

    z_total = z1_own.at[y]
    x_raw[...] = token_t[...].T.reshape(x_raw.shape)
    reduce_over_kv(
        norm_gain, w1, n_main, 2 * heads, True, z1_pair, z1_own, z1_got, z1_send, z1_recv, (p1_s, p1_r, a_s, a_r), z_total
    )
    with jax.named_scope("gates"):
        gates = tile_of(z_total, z1_recv, n_main)
        scale1 = lax.rsqrt(gates[:, 2 * heads : 2 * heads + 1] / n_feats + 1e-06)
        query = scale1 * total_of(z_total, z1_recv, 0, dq) * DQK ** (-0.5)
        key = scale1 * total_of(z_total, z1_recv, dq, dk)
        value = scale1 * total_of(z_total, z1_recv, dq + dk, dv)
        outgate = scale1 * total_of(z_total, z1_recv, dq + dk + dv, dv)
        igate = scale1 * gates[:, :heads]
        forget = scale1 * gates[:, heads : 2 * heads]
        lforget = jnp.minimum(forget, 0.0) - jnp.log1p(jnp.exp(-jnp.abs(forget)))
        loads["stab"].wait()
        loads["norm"].wait()
        loads["mem"].wait()
        held = lforget + stab[...].T
        new_stab = jnp.maximum(held, igate)
        newstab_ref[...] = new_stab.T
        decay = jnp.exp(held - new_stab)
        inflow = jnp.exp(igate - new_stab)
        floor = jnp.exp(-new_stab)
    with jax.named_scope("readout"):
        query_t = query.T
        for s in range(own):
            for h in range(heads):
                column = query_t[h * DQK : (h + 1) * DQK, s : s + 1]
                numer[s : s + 1, h * DV : (h + 1) * DV] = jnp.sum(column * mem[s, h], axis=0, keepdims=True)
    with jax.named_scope("norm"):
        for h in range(heads):
            q, k = query[:, h * DQK : (h + 1) * DQK], key[:, h * DQK : (h + 1) * DQK]
            keep, add = decay[:, h : h + 1], inflow[:, h : h + 1]
            new_norm = keep * norm[:, h, :] + add * k
            newnorm_ref[:, h, :] = new_norm
            denom = jnp.maximum(jnp.abs(jnp.sum(q * new_norm, axis=1, keepdims=True)), floor[:, h : h + 1])
            at = slice(h * DV, (h + 1) * DV)
            top = keep * numer[:, at] + (add * jnp.sum(q * k, axis=1, keepdims=True)) * value[:, at]
            gated[rows(kv, own), at] = (jax.nn.sigmoid(outgate[:, at]) * (top / denom)).astype(BF16)
    finish = gather_over_kv(gated, (g_s, g_r, gf_s, gf_r))

    with jax.named_scope("newmem"):
        spread = jnp.concatenate([jnp.broadcast_to(inflow[:, h : h + 1], (own, DQK)) for h in range(heads)], axis=1)
        key_t = (key * spread).T
        for s in range(own):
            for h in range(heads):
                column = key_t[h * DQK : (h + 1) * DQK, s : s + 1]
                mem[s, h] = decay[s : s + 1, h : h + 1] * mem[s, h] + column * value[s : s + 1, h * DV : (h + 1) * DV]
    put = pltpu.make_async_copy(mem, newmem_h, local_sem.at[12])
    put.start()
    with jax.named_scope("wait_gated"):
        finish()

    with jax.named_scope("mixdot"):
        partial = lax.dot_general(wmix_t[...], gated[...], (((1,), (1,)), ((), ())), preferred_element_type=F32)
    with jax.named_scope("mixrs"):
        total = sum_over_tp(partial, mix_send, mix_recv, (m_s, m_r))
    mixed = (token_t[rows(tp, mine), :].astype(F32) + total).astype(BF16)
    mixed_t[rows(tp, mine), :] = mixed
    for d in far_first(n_tp):
        part = mixed_t.at[rows(tp, mine), :]
        send(part, part, x_s.at[d], x_r.at[d], {"tp": tp_of(d)})
    with jax.named_scope("wait_mixed"):
        for at, _ in ff_chunks(n_ff):
            loads[f"gate{at}"].wait()
            loads[f"up{at}"].wait()
        for d in near_first(n_tp):
            arrive(mixed_t.at[rows(from_tp(d), mine), :], x_s.at[d], x_r.at[d], {"tp": tp_of(d)})

    x_raw[...] = mixed_t[...].T.reshape(x_raw.shape)
    chunks = ff_chunks(n_ff)
    order = [len(chunks) - 1] + list(range(len(chunks) - 1))
    wide_lane = lax.broadcasted_iota(jnp.int32, (half_rows, LANES), 1)
    small_lane = lax.broadcasted_iota(jnp.int32, (own, LANES), 1)

    def project_chunks(core_of, ours):
        wide = x_raw[:, core_of].reshape(half_rows, feats).astype(F32)
        normed = (wide * ffn_gain[...].astype(F32)[None, :]).astype(BF16)
        squares = jnp.sum(wide * wide, axis=1, keepdims=True)
        tile = jnp.broadcast_to(squares, (half_rows, LANES))
        if ours:
            z2_own[:, :, 2 * n_ff :] = tile.reshape(n_y, own, LANES)
        else:
            z2_pair[:, :, 2 * n_ff :] = hi_lo(tile, wide_lane).reshape(n_y, own, LANES)
        for c in order:
            at, size = chunks[c]
            for start in (2 * at, 2 * at + size):
                z = jnp.dot(normed, w2[:, start : start + size], preferred_element_type=F32)
                if ours:
                    z2_own[:, :, start : start + size] = z.reshape(n_y, own, size)
                else:
                    z2_pair[:, :, start : start + size] = z.astype(BF16).reshape(n_y, own, size)
            if not ours:
                part = pl.ds(2 * at, width_of(c))
                send(z2_pair.at[:, :, part], z2_got.at[:, :, part], p2_s.at[c], p2_r.at[c], {"kv": partner})

    def width_of(c):
        return 2 * chunks[c][1] + (LANES if c == len(chunks) - 1 else 0)

    def spans(c):
        at, size = chunks[c]
        return [(2 * at, size, False), (2 * at + size, size, False)] + (
            [(2 * n_ff, LANES, True)] if c == len(chunks) - 1 else []
        )

    def plain(tile, is_square):
        tile = tile.astype(F32)
        if is_square:
            tile = tile + jnp.concatenate([tile[:, HALF:], tile[:, :HALF]], axis=1)
        return tile

    def add_up(c, dest, received, put):
        for at, size, is_square in spans(c):
            value = z2_own[dest, :, at : at + size] + plain(z2_got[dest, :, at : at + size], is_square)
            for slot in received:
                value = value + plain(z2_recv[slot, :, at : at + size], is_square)
            put(at, size, is_square, value)

    def pass_on(c, dest, received, slot, hops):
        def put(at, size, is_square, value):
            z2_send[slot, :, at : at + size] = hi_lo(value, small_lane) if is_square else value.astype(BF16)

        add_up(c, dest, received, put)
        part = pl.ds(2 * chunks[c][0], width_of(c))
        where = {"kv": 2 * lax.rem(y + n_y + hops, n_y) + core}
        send(z2_send.at[slot, :, part], z2_recv.at[slot, :, part], b_s.at[slot, c], b_r.at[slot, c], where)

    def take(c, slot):
        part = pl.ds(2 * chunks[c][0], width_of(c))
        target = z2_recv.at[slot, :, part]
        arrive(target, b_s.at[slot, c], b_r.at[slot, c], {"kv": partner})

    far, short = n_y // 2, n_y // 2 - 1
    with jax.named_scope("proj2a"):
        project_chunks(other, False)
    with jax.named_scope("proj2b"):
        project_chunks(core, True)

    def way(c):
        return 1 if c % 2 == 0 else -1

    def slot_of(sign, step):
        return step if sign == 1 else short + step

    for c in order:
        with jax.named_scope(f"ring#s=1#c={c}"):
            part = pl.ds(2 * chunks[c][0], width_of(c))
            arrive(z2_got.at[:, :, part], p2_s.at[c], p2_r.at[c], {"kv": partner})
            pass_on(c, lax.rem(y + far, n_y), [], 0, 2 * way(c))
            for sign in (1, -1):
                pass_on(c, lax.rem(y + n_y + sign * short, n_y), [], slot_of(sign, 1), sign)
    for step in range(2, short + 1):
        for c in order:
            with jax.named_scope(f"ring#s={step}#c={c}"):
                for sign in (-way(c), way(c)):
                    received = [slot_of(sign, step - 1)]
                    if step == 2 and sign == way(c):
                        received.append(0)
                    for slot in received:
                        take(c, slot)
                    pass_on(c, lax.rem(y + n_y + sign * (short + 1 - step), n_y), received, slot_of(sign, step), sign)

    scale2 = None
    for c in order:
        at, size = chunks[c]
        with jax.named_scope(f"hidden#c={c}"):
            parts = []
            received = [slot_of(sign, short) for sign in (1, -1)]
            for slot in received:
                take(c, slot)
            add_up(c, y, received, lambda at, size, is_square, value: parts.append(value))
            if scale2 is None:
                scale2 = lax.rsqrt(parts[2][:, :1] / n_feats + 1e-06)
            gate, up = scale2 * parts[0], scale2 * parts[1]
            hidden[rows(kv, own), at : at + size] = (gate * jax.nn.sigmoid(gate) * up).astype(BF16)
            part = hidden.at[rows(kv, own), pl.ds(at, size)]
            for d in far_first(n_y):
                send(part, part, h_s.at[d, c], h_r.at[d, c], {"kv": 2 * y_of(d) + core})
            send(part, part, hf_s.at[0, c], hf_r.at[0, c], {"kv": partner})

    def pass_to_partner(c):
        at, size = chunks[c]
        with jax.named_scope(f"pass#c={c}"):
            for d in near_first(n_y):
                got = hidden.at[rows(2 * from_y(d) + core, own), pl.ds(at, size)]
                arrive(got, h_s.at[d, c], h_r.at[d, c], {"kv": 2 * y_of(d) + core})
                send(got, got, hf_s.at[d, c], hf_r.at[d, c], {"kv": partner})

    def down_part(c):
        at, size = chunks[c]
        with jax.named_scope(f"down#c={c}"):
            for d in [0] + near_first(n_y):
                target = hidden.at[rows(2 * from_y(d) + other, own), pl.ds(at, size)]
                arrive(target, hf_s.at[d, c], hf_r.at[d, c], {"kv": partner})
            return lax.dot_general(
                wd_t[:, at : at + size], hidden[:, at : at + size], (((1,), (1,)), ((), ())), preferred_element_type=F32
            )

    pass_to_partner(order[0])
    for i, c in enumerate(order):
        if i + 1 < len(order):
            pass_to_partner(order[i + 1])
        product = down_part(c)
        if i == 0:
            down_sum[...] = product
        elif i + 1 < len(order):
            down_sum[...] += product
    with jax.named_scope("downrs"):
        total = sum_over_tp(down_sum[...] + product, down_send, down_recv, (d_s, d_r))
    out_ref[...] = (mixed_t[rows(tp, mine), :].astype(F32) + total).astype(BF16)
    put.wait()
    for copy in sent:
        copy.wait_send()


def copy_kernel(pieces, *refs):
    count = len(pieces)
    sources, targets, held, sem = refs[:count], refs[count : 2 * count], refs[2 * count : 3 * count], refs[3 * count]
    steps, at = [], 0
    for source, target, buffer, n in zip(sources, targets, held, pieces):
        size = source.shape[0] // n
        for i in range(n):
            part = pl.ds(i * size, size)
            steps.append((
                pltpu.make_async_copy(source.at[part], buffer.at[part], sem.at[0, at]),
                pltpu.make_async_copy(buffer.at[part], target.at[part], sem.at[1, at]),
            ))
            at += 1
    for take, _ in steps:
        take.start()
    for take, put in steps:
        take.wait()
        put.start()
    for _, put in steps:
        put.wait()


def hand_over(*arrays):
    pieces = [4 if a.ndim == 4 else 1 for a in arrays]
    hbm = pl.BlockSpec(memory_space=pltpu.HBM)
    return pl.pallas_call(
        functools.partial(copy_kernel, pieces),
        out_shape=tuple(jax.ShapeDtypeStruct(a.shape, a.dtype) for a in arrays),
        in_specs=[hbm] * len(arrays),
        out_specs=(hbm,) * len(arrays),
        scratch_shapes=[pltpu.VMEM(a.shape, a.dtype) for a in arrays] + [pltpu.SemaphoreType.DMA((2, sum(pieces)))],
        compiler_params=pltpu.CompilerParams(vmem_limit_bytes=67_043_328),
        name="hand_over",
    )(*arrays)


def shards(n_kv, n_tp, tokens, norm_gain, w_query, w_key, w_value, w_outgate, w_input_gate, w_forget_gate, memory, normalizer, stabilizer, w_mix_out, ffn_gain, w_gate, w_up, w_down):
    seqs, mine = tokens.shape
    feats = norm_gain.shape[0]
    n_y = n_kv // 2
    own = memory.shape[0]
    dv = w_value.shape[1]
    n1 = w_query.shape[1] + w_key.shape[1] + 2 * dv + LANES
    n_ff = w_gate.shape[1]
    n2 = 2 * n_ff + LANES
    out_feats = w_mix_out.shape[1]
    hbm = pl.BlockSpec(memory_space=pltpu.HBM)
    vmem = pl.BlockSpec(memory_space=pltpu.VMEM)
    dma = pltpu.SemaphoreType.DMA
    n_chunks = len(ff_chunks(n_ff))
    ys, xs, one, per_chunk = dma((n_y,)), dma((n_tp,)), dma, dma((n_y, n_chunks))
    out_t, new_memory, new_normalizer, new_stabilizer = pl.pallas_call(
        functools.partial(layer_kernel, n_kv, n_tp),
        out_shape=(
            jax.ShapeDtypeStruct((mine, seqs), BF16),
            jax.ShapeDtypeStruct(memory.shape, F32),
            jax.ShapeDtypeStruct(normalizer.shape, F32),
            jax.ShapeDtypeStruct(stabilizer.shape[::-1], F32),
        ),
        in_specs=[hbm, vmem] + [hbm] * 10 + [vmem] + [hbm] * 3,
        out_specs=(vmem, hbm, vmem, vmem),
        scratch_shapes=[
            pltpu.VMEM((feats, n1), BF16),
            pltpu.VMEM((2 * w_input_gate.shape[1], feats), BF16),
            pltpu.VMEM(memory.shape, F32),
            pltpu.VMEM(normalizer.shape, F32),
            pltpu.VMEM(stabilizer.shape[::-1], F32),
            pltpu.VMEM(w_mix_out.shape, BF16),
            pltpu.VMEM(w_mix_out.shape[::-1], BF16),
            pltpu.VMEM((feats, 2 * n_ff), BF16),
            pltpu.VMEM(w_down.shape, BF16),
            pltpu.VMEM(w_down.shape[::-1], BF16),
            pltpu.VMEM((feats, seqs), BF16),
            pltpu.VMEM((n_y, 2, own, feats), BF16),
            pltpu.VMEM((n_y, own, n1), BF16),
            pltpu.VMEM((n_y, own, n1), F32),
            pltpu.VMEM((n_y, own, n1), BF16),
            pltpu.VMEM((n_y, own, n1), BF16),
            pltpu.VMEM((n_y, own, n1), BF16),
            pltpu.VMEM((own, dv), F32),
            pltpu.VMEM((seqs, dv), BF16),
            pltpu.VMEM((n_tp, mine, seqs), BF16),
            pltpu.VMEM((n_tp, mine, seqs), BF16),
            pltpu.VMEM((out_feats, seqs), BF16),
            pltpu.VMEM((n_y, own, n2), BF16),
            pltpu.VMEM((n_y, own, n2), F32),
            pltpu.VMEM((n_y, own, n2), BF16),
            pltpu.VMEM((n_y, own, n2), BF16),
            pltpu.VMEM((n_y, own, n2), BF16),
            pltpu.VMEM((seqs, n_ff), BF16),
            pltpu.VMEM((out_feats, seqs), F32),
            pltpu.VMEM((n_tp, mine, seqs), BF16),
            pltpu.VMEM((n_tp, mine, seqs), BF16),
            dma((13 + 2 * len(ff_chunks(n_ff)),)),
            xs, xs,
            one, one, ys, ys,
            ys, ys, ys, ys,
            xs, xs,
            xs, xs,
            dma((n_chunks,)), dma((n_chunks,)), per_chunk, per_chunk,
            per_chunk, per_chunk, per_chunk, per_chunk,
            xs, xs,
        ],
        compiler_params=pltpu.CompilerParams(collective_id=0, has_side_effects=True, vmem_limit_bytes=67_043_328),
        name="layer",
    )(
        tokens.T, norm_gain, w_query, w_key, w_value, w_outgate, w_input_gate.T, w_forget_gate.T,
        memory, normalizer, stabilizer.T, w_mix_out, ffn_gain, w_gate, w_up, w_down,
    )
    out_t, new_memory, new_normalizer, new_stabilizer = hand_over(out_t, new_memory, new_normalizer, new_stabilizer)
    return out_t.T, new_memory, new_normalizer, new_stabilizer.T


def solution(mesh):
    in_specs = (
        P("grp", ("kv", "tp")),
        P("kv"),
        P("kv", "tp"),
        P("kv", "tp"),
        P("kv", "tp"),
        P("kv", "tp"),
        P("kv", None),
        P("kv", None),
        P(("grp", "kv"), "tp", None, None),
        P(("grp", "kv"), "tp", None),
        P(("grp", "kv"), "tp"),
        P("tp", "kv"),
        P("kv"),
        P("kv", "tp"),
        P("kv", "tp"),
        P("tp", "kv"),
    )
    out_specs = (
        P("grp", ("kv", "tp")),
        P(("grp", "kv"), "tp", None, None),
        P(("grp", "kv"), "tp", None),
        P(("grp", "kv"), "tp"),
    )
    body = functools.partial(shards, mesh.shape["kv"], mesh.shape["tp"])
    return jax.shard_map(body, mesh=mesh, in_specs=in_specs, out_specs=out_specs, check_vma=False)
```

```python
import functools

import jax
import jax.numpy as jnp
from jax import lax
from jax.experimental import pallas as pl
from jax.experimental.pallas import tpu as pltpu
from jax.sharding import PartitionSpec as P

DQK = 64
DV = 128
LANES = 128
HALF = LANES // 2
FF_CHUNK = 3 * LANES
F32 = jnp.float32
BF16 = jnp.bfloat16
MESH = pl.DeviceIdType.MESH


def far_first(count):
    return sorted(range(1, count), key=lambda d: -min(d, count - d))


def near_first(count):
    return far_first(count)[::-1]


def column_pieces(width, step=256):
    return [(at, min(step, width - at)) for at in range(0, width, step)]


def ff_chunks(width):
    first = width % FF_CHUNK or FF_CHUNK
    return [(0, first)] + [(at, FF_CHUNK) for at in range(first, width, FF_CHUNK)]


def with_ends(sizes_of_chunks):
    at, chunks = 0, []
    for sizes in sizes_of_chunks:
        chunk = []
        for size in sizes:
            chunk.append((at, size))
            at += size
        chunks.append(chunk)
    return chunks


def hi_lo(values, lane):
    high = values.astype(BF16).astype(F32)
    return jnp.where(lane < HALF, high, values - high).astype(BF16)


def layer_kernel(
    n_kv, n_tp,
    tokens_h, norm_gain, wq_h, wk_h, wv_h, wo_h, wi_h, wf_h, mem_h, norm_h, stab_h, wmix_h, ffn_gain, wg_h, wu_h, wd_h,
    out_ref, newmem_h, newnorm_ref, newstab_ref,
    w1, wgates, mem, norm, stab, wmix, wmix_t, w2, wd, wd_t,
    token_t, x_raw, z1_pair, z1_own, z1_got, z1_send, z1_recv,
    numer, gated, mix_send, mix_recv, mixed_t, z2_pair, z2_own, z2_got, z2_send, z2_recv, hidden, down_sum, down_send, down_recv,
    local_sem, tok_s, tok_r, p1_s, p1_r, a_s, a_r, g_s, g_r, gf_s, gf_r, m_s, m_r, x_s, x_r, p2_s, p2_r, b_s, b_r, h_s, h_r, hf_s, hf_r, d_s, d_r,
):
    kv, tp = lax.axis_index("kv"), lax.axis_index("tp")
    n_y = n_kv // 2
    core, y = lax.rem(kv, 2), kv // 2
    other = 1 - core
    partner = 2 * y + other
    own = mem.shape[0]
    heads = mem.shape[1]
    feats = token_t.shape[0]
    mine = tokens_h.shape[0]
    half_rows = n_y * own
    n_feats = feats * n_kv

    def y_of(d):
        return lax.rem(y + d, n_y)

    def from_y(d):
        return lax.rem(y + n_y - d, n_y)

    def tp_of(d):
        return lax.rem(tp + d, n_tp)

    def from_tp(d):
        return lax.rem(tp + n_tp - d, n_tp)

    def rows(index, size):
        return pl.ds(pl.multiple_of(index * size, size), size)

    barrier = pltpu.get_barrier_semaphore()
    for d in far_first(n_tp):
        pl.semaphore_signal(barrier, inc=1, device_id={"tp": tp_of(d)}, device_id_type=MESH)
    for d in far_first(n_y):
        pl.semaphore_signal(barrier, inc=1, device_id={"kv": 2 * y_of(d) + core}, device_id_type=MESH)
    pl.semaphore_signal(barrier, inc=1, device_id={"kv": partner}, device_id_type=MESH)

    dq, dk, dv = wq_h.shape[1], wk_h.shape[1], wv_h.shape[1]
    n_ff = wg_h.shape[1]
    n_gate = wi_h.shape[0]
    loads = {}
    for i, (name, source, target) in enumerate((
        ("tokens", tokens_h, token_t.at[rows(tp, mine), :]),
        ("wi", wi_h, wgates.at[pl.ds(0, n_gate), :]),
        ("wf", wf_h, wgates.at[pl.ds(n_gate, n_gate), :]),
        ("wq", wq_h, w1.at[:, pl.ds(LANES, dq)]),
        ("wk", wk_h, w1.at[:, pl.ds(LANES + dq, dk)]),
        ("wv", wv_h, w1.at[:, pl.ds(LANES + dq + dk, dv)]),
        ("wo", wo_h, w1.at[:, pl.ds(LANES + dq + dk + dv, dv)]),
        ("mix", wmix_h, wmix),
        ("down", wd_h, wd),
        ("mem", mem_h, mem),
        ("norm", norm_h, norm),
        ("stab", stab_h, stab),
    ) + tuple(
        (f"{name}{at}", source.at[:, pl.ds(at, size)], w2.at[:, pl.ds(LANES + 2 * at + shift * size, size)])
        for at, size in ff_chunks(n_ff)
        for shift, (name, source) in enumerate((("gate", wg_h), ("up", wu_h)))
    )):
        loads[name] = pltpu.make_async_copy(source, target, local_sem.at[i + (i >= 12)])
        loads[name].start()
    sent = []

    def send(source, target, send_sem, recv_sem, where):
        copy = pltpu.make_async_remote_copy(
            src_ref=source, dst_ref=target, send_sem=send_sem, recv_sem=recv_sem, device_id=where, device_id_type=MESH
        )
        copy.start()
        sent.append(copy)

    def arrive(target, send_sem, recv_sem, where):
        pltpu.make_async_remote_copy(
            src_ref=target, dst_ref=target, send_sem=send_sem, recv_sem=recv_sem, device_id=where, device_id_type=MESH
        ).wait_recv()

    loads["tokens"].wait()
    with jax.named_scope("barrier"):
        pl.semaphore_wait(barrier, (n_tp - 1) + (n_y - 1) + 1)
    for d in far_first(n_tp):
        part = token_t.at[rows(tp, mine), :]
        send(part, part, tok_s.at[d], tok_r.at[d], {"tp": tp_of(d)})

    loads["wi"].wait()
    loads["wf"].wait()
    with jax.named_scope("prep"):
        lane_w = lax.rem(lax.broadcasted_iota(jnp.int32, (2 * n_gate, LANES), 1), HALF)
        row_w = lax.broadcasted_iota(jnp.int32, (2 * n_gate, LANES), 0)
        is_f = row_w // n_gate
        head = row_w - is_f * n_gate - tp * heads
        pick = jnp.where((head >= 0) & (head < heads) & (lane_w == head + heads * is_f), 1.0, 0.0).astype(BF16)
        w1[:, :LANES] = lax.dot_general(
            wgates[...], pick, (((0,), (0,)), ((), ())), preferred_element_type=F32
        ).astype(BF16)

        loads["mix"].wait()
        wmix_t[...] = wmix[...].T
        loads["down"].wait()
        for at, width in column_pieces(wd.shape[0]):
            wd_t[:, at : at + width] = wd[at : at + width, :].T
        for name in ("wq", "wk", "wv", "wo"):
            loads[name].wait()

    with jax.named_scope("wait_tok"):
        for d in near_first(n_tp):
            arrive(token_t.at[rows(from_tp(d), mine), :], tok_s.at[d], tok_r.at[d], {"tp": tp_of(d)})

    lane = lax.broadcasted_iota(jnp.int32, (half_rows, LANES), 1)

    small_lane = lax.broadcasted_iota(jnp.int32, (own, LANES), 1)
    far, short = n_y // 2, n_y // 2 - 1

    def slot_of(sign, step):
        return step if sign == 1 else short + step

    def sum_over_kv(name, gain, weights, square_lane, chunks, pair, own_z, got, out, into, sems):
        p_s, p_r, r_s, r_r = sems

        def part_of(c):
            return pl.ds(chunks[c][0][0], sum(size for _, size in chunks[c]))

        def project(core_of, ours):
            wide = x_raw[:, core_of].reshape(half_rows, feats).astype(F32)
            normed = (wide * gain[...].astype(F32)[None, :]).astype(BF16)
            squares = jnp.sum(wide * wide, axis=1, keepdims=True)
            for c, chunk in enumerate(chunks):
                for at, size in chunk:
                    if at == 0 and square_lane is None:
                        z = jnp.broadcast_to(squares, (half_rows, LANES))
                    else:
                        z = jnp.dot(normed, weights[:, at : at + size], preferred_element_type=F32)
                        if at == 0:
                            z = jnp.where(lax.rem(lane, HALF) == square_lane, squares, z)
                    if ours:
                        own_z[:, :, at : at + size] = z.reshape(n_y, own, size)
                    else:
                        z = hi_lo(z, lane) if at == 0 else z.astype(BF16)
                        pair[:, :, at : at + size] = z.reshape(n_y, own, size)
                if not ours:
                    send(pair.at[:, :, part_of(c)], got.at[:, :, part_of(c)], p_s.at[c], p_r.at[c], {"kv": partner})

        def plain(tile, at):
            tile = tile.astype(F32)
            if at == 0:
                tile = tile + jnp.concatenate([tile[:, HALF:], tile[:, :HALF]], axis=1)
            return tile

        def add_up(c, dest, received):
            for at, size in chunks[c]:
                value = own_z[dest, :, at : at + size] + plain(got[dest, :, at : at + size], at)
                for slot in received:
                    value = value + plain(into[slot, :, at : at + size], at)
                yield at, size, value

        def pass_on(c, dest, received, slot, hops):
            for at, size, value in add_up(c, dest, received):
                out[slot, :, at : at + size] = hi_lo(value, small_lane) if at == 0 else value.astype(BF16)
            where = {"kv": 2 * lax.rem(y + n_y + hops, n_y) + core}
            send(out.at[slot, :, part_of(c)], into.at[slot, :, part_of(c)], r_s.at[slot, c], r_r.at[slot, c], where)

        def take(c, slot):
            arrive(into.at[slot, :, part_of(c)], r_s.at[slot, c], r_r.at[slot, c], {"kv": partner})

        def way(c):
            return 1 if c % 2 == 0 else -1

        with jax.named_scope(f"{name}_proj_a"):
            project(other, False)
        with jax.named_scope(f"{name}_proj_b"):
            project(core, True)
        for c in range(len(chunks)):
            with jax.named_scope(f"{name}_ring#s=1#c={c}"):
                arrive(got.at[:, :, part_of(c)], p_s.at[c], p_r.at[c], {"kv": partner})
                pass_on(c, lax.rem(y + far, n_y), [], 0, 2 * way(c))
                for sign in (1, -1):
                    pass_on(c, lax.rem(y + n_y + sign * short, n_y), [], slot_of(sign, 1), sign)
        for step in range(2, short + 1):
            for c in range(len(chunks)):
                with jax.named_scope(f"{name}_ring#s={step}#c={c}"):
                    for sign in (-way(c), way(c)):
                        received = [slot_of(sign, step - 1)]
                        if step == 2 and sign == way(c):
                            received.append(0)
                        for slot in received:
                            take(c, slot)
                        dest = lax.rem(y + n_y + sign * (short + 1 - step), n_y)
                        pass_on(c, dest, received, slot_of(sign, step), sign)

        def finish(c):
            received = [slot_of(sign, short) for sign in (1, -1)]
            for slot in received:
                take(c, slot)
            return [value for _, _, value in add_up(c, y, received)]

        return finish

    def gather_over_kv(buffer, sems):
        r_s, r_r, f_s, f_r = sems
        part = buffer.at[rows(kv, own), :]
        for d in far_first(n_y):
            send(part, part, r_s.at[d], r_r.at[d], {"kv": 2 * y_of(d) + core})
        send(part, part, f_s.at[0], f_r.at[0], {"kv": partner})

        def finish():
            for d in near_first(n_y):
                got = buffer.at[rows(2 * from_y(d) + core, own), :]
                arrive(got, r_s.at[d], r_r.at[d], {"kv": 2 * y_of(d) + core})
                send(got, got, f_s.at[d], f_r.at[d], {"kv": partner})
            for d in [0] + near_first(n_y):
                arrive(buffer.at[rows(2 * from_y(d) + other, own), :], f_s.at[d], f_r.at[d], {"kv": partner})

        return finish

    def sum_over_tp(partial, out, into, sems):
        s, r = sems
        out[...] = partial.astype(BF16).reshape(n_tp, mine, partial.shape[1])
        for d in far_first(n_tp):
            send(out.at[tp_of(d)], into.at[d], s.at[d], r.at[d], {"tp": tp_of(d)})
        total = out[tp].astype(F32)
        for d in near_first(n_tp):
            arrive(into.at[d], s.at[d], r.at[d], {"tp": tp_of(d)})
            total = total + into[d].astype(F32)
        return total

    x_raw[...] = token_t[...].T.reshape(x_raw.shape)
    sums = sum_over_kv(
        "in", norm_gain, w1, 2 * heads, with_ends([[LANES, dq, dk], [dv], [dv]]),
        z1_pair, z1_own, z1_got, z1_send, z1_recv, (p1_s, p1_r, a_s, a_r),
    )
    gates, query, key = sums(0)
    scale1 = lax.rsqrt(gates[:, 2 * heads : 2 * heads + 1] / n_feats + 1e-06)
    query = scale1 * query * DQK ** (-0.5)
    key = scale1 * key
    igate = scale1 * gates[:, :heads]
    forget = scale1 * gates[:, heads : 2 * heads]
    lforget = jnp.minimum(forget, 0.0) - jnp.log1p(jnp.exp(-jnp.abs(forget)))
    loads["stab"].wait()
    loads["norm"].wait()
    loads["mem"].wait()
    held = lforget + stab[...].T
    new_stab = jnp.maximum(held, igate)
    newstab_ref[...] = new_stab.T
    decay = jnp.exp(held - new_stab)
    inflow = jnp.exp(igate - new_stab)
    floor = jnp.exp(-new_stab)
    with jax.named_scope("readout"):
        query_t = query.T
        for s in range(own):
            for h in range(heads):
                column = query_t[h * DQK : (h + 1) * DQK, s : s + 1]
                numer[s : s + 1, h * DV : (h + 1) * DV] = jnp.sum(column * mem[s, h], axis=0, keepdims=True)
    with jax.named_scope("norm"):
        parts = []
        for h in range(heads):
            q, k = query[:, h * DQK : (h + 1) * DQK], key[:, h * DQK : (h + 1) * DQK]
            keep, add = decay[:, h : h + 1], inflow[:, h : h + 1]
            new_norm = keep * norm[:, h, :] + add * k
            newnorm_ref[:, h, :] = new_norm
            denom = jnp.maximum(jnp.abs(jnp.sum(q * new_norm, axis=1, keepdims=True)), floor[:, h : h + 1])
            parts.append((keep * numer[:, h * DV : (h + 1) * DV], add * jnp.sum(q * k, axis=1, keepdims=True), denom))
    with jax.named_scope("value"):
        (value,) = sums(1)
        value = scale1 * value
        readout = [
            (top + weight * value[:, h * DV : (h + 1) * DV]) / denom for h, (top, weight, denom) in enumerate(parts)
        ]
    with jax.named_scope("outgate"):
        (outgate,) = sums(2)
        outgate = scale1 * outgate
        for h in range(heads):
            at = slice(h * DV, (h + 1) * DV)
            gated[rows(kv, own), at] = (jax.nn.sigmoid(outgate[:, at]) * readout[h]).astype(BF16)
    finish = gather_over_kv(gated, (g_s, g_r, gf_s, gf_r))

    with jax.named_scope("newmem"):
        spread = jnp.concatenate([jnp.broadcast_to(inflow[:, h : h + 1], (own, DQK)) for h in range(heads)], axis=1)
        key_t = (key * spread).T
        for s in range(own):
            for h in range(heads):
                column = key_t[h * DQK : (h + 1) * DQK, s : s + 1]
                mem[s, h] = decay[s : s + 1, h : h + 1] * mem[s, h] + column * value[s : s + 1, h * DV : (h + 1) * DV]
    put = pltpu.make_async_copy(mem, newmem_h, local_sem.at[12])
    put.start()
    with jax.named_scope("wait_gated"):
        finish()

    with jax.named_scope("mixdot"):
        partial = lax.dot_general(wmix_t[...], gated[...], (((1,), (1,)), ((), ())), preferred_element_type=F32)
    with jax.named_scope("mixrs"):
        total = sum_over_tp(partial, mix_send, mix_recv, (m_s, m_r))
    mixed = (token_t[rows(tp, mine), :].astype(F32) + total).astype(BF16)
    mixed_t[rows(tp, mine), :] = mixed
    for d in far_first(n_tp):
        part = mixed_t.at[rows(tp, mine), :]
        send(part, part, x_s.at[d], x_r.at[d], {"tp": tp_of(d)})
    with jax.named_scope("wait_mixed"):
        for at, _ in ff_chunks(n_ff):
            loads[f"gate{at}"].wait()
            loads[f"up{at}"].wait()
        for d in near_first(n_tp):
            arrive(mixed_t.at[rows(from_tp(d), mine), :], x_s.at[d], x_r.at[d], {"tp": tp_of(d)})

    x_raw[...] = mixed_t[...].T.reshape(x_raw.shape)
    chunks = ff_chunks(n_ff)
    sizes = [[size, size] for _, size in chunks]
    sizes[0] = [LANES] + sizes[0]
    sums = sum_over_kv(
        "ff", ffn_gain, w2, None, with_ends(sizes), z2_pair, z2_own, z2_got, z2_send, z2_recv, (p2_s, p2_r, b_s, b_r)
    )

    scale2 = None
    for c, (at, size) in enumerate(chunks):
        with jax.named_scope(f"hidden#c={c}"):
            *squares, gate, up = sums(c)
            if c == 0:
                scale2 = lax.rsqrt(squares[0][:, :1] / n_feats + 1e-06)
            gate, up = scale2 * gate, scale2 * up
            hidden[rows(kv, own), at : at + size] = (gate * jax.nn.sigmoid(gate) * up).astype(BF16)
            part = hidden.at[rows(kv, own), pl.ds(at, size)]
            for d in far_first(n_y):
                send(part, part, h_s.at[d, c], h_r.at[d, c], {"kv": 2 * y_of(d) + core})
            send(part, part, hf_s.at[0, c], hf_r.at[0, c], {"kv": partner})

    def pass_to_partner(c):
        at, size = chunks[c]
        with jax.named_scope(f"pass#c={c}"):
            for d in near_first(n_y):
                got = hidden.at[rows(2 * from_y(d) + core, own), pl.ds(at, size)]
                arrive(got, h_s.at[d, c], h_r.at[d, c], {"kv": 2 * y_of(d) + core})
                send(got, got, hf_s.at[d, c], hf_r.at[d, c], {"kv": partner})

    def down_part(c):
        at, size = chunks[c]
        with jax.named_scope(f"down#c={c}"):
            for d in [0] + near_first(n_y):
                target = hidden.at[rows(2 * from_y(d) + other, own), pl.ds(at, size)]
                arrive(target, hf_s.at[d, c], hf_r.at[d, c], {"kv": partner})
            return lax.dot_general(
                wd_t[:, at : at + size], hidden[:, at : at + size], (((1,), (1,)), ((), ())), preferred_element_type=F32
            )

    pass_to_partner(0)
    for c in range(len(chunks)):
        if c + 1 < len(chunks):
            pass_to_partner(c + 1)
        product = down_part(c)
        if c == 0:
            down_sum[...] = product
        elif c + 1 < len(chunks):
            down_sum[...] += product
    with jax.named_scope("downrs"):
        total = sum_over_tp(down_sum[...] + product, down_send, down_recv, (d_s, d_r))
    out_ref[...] = (mixed_t[rows(tp, mine), :].astype(F32) + total).astype(BF16)
    put.wait()
    for copy in sent:
        copy.wait_send()


def copy_kernel(pieces, *refs):
    count = len(pieces)
    sources, targets, held, sem = refs[:count], refs[count : 2 * count], refs[2 * count : 3 * count], refs[3 * count]
    steps, at = [], 0
    for source, target, buffer, n in zip(sources, targets, held, pieces):
        size = source.shape[0] // n
        for i in range(n):
            part = pl.ds(i * size, size)
            steps.append((
                pltpu.make_async_copy(source.at[part], buffer.at[part], sem.at[0, at]),
                pltpu.make_async_copy(buffer.at[part], target.at[part], sem.at[1, at]),
            ))
            at += 1
    for take, _ in steps:
        take.start()
    for take, put in steps:
        take.wait()
        put.start()
    for _, put in steps:
        put.wait()


def hand_over(*arrays):
    pieces = [4 if a.ndim == 4 else 1 for a in arrays]
    hbm = pl.BlockSpec(memory_space=pltpu.HBM)
    return pl.pallas_call(
        functools.partial(copy_kernel, pieces),
        out_shape=tuple(jax.ShapeDtypeStruct(a.shape, a.dtype) for a in arrays),
        in_specs=[hbm] * len(arrays),
        out_specs=(hbm,) * len(arrays),
        scratch_shapes=[pltpu.VMEM(a.shape, a.dtype) for a in arrays] + [pltpu.SemaphoreType.DMA((2, sum(pieces)))],
        compiler_params=pltpu.CompilerParams(vmem_limit_bytes=67_043_328),
        name="hand_over",
    )(*arrays)


def shards(n_kv, n_tp, tokens, norm_gain, w_query, w_key, w_value, w_outgate, w_input_gate, w_forget_gate, memory, normalizer, stabilizer, w_mix_out, ffn_gain, w_gate, w_up, w_down):
    seqs, mine = tokens.shape
    feats = norm_gain.shape[0]
    n_y = n_kv // 2
    own = memory.shape[0]
    dv = w_value.shape[1]
    n1 = w_query.shape[1] + w_key.shape[1] + 2 * dv + LANES
    n_ff = w_gate.shape[1]
    n2 = 2 * n_ff + LANES
    out_feats = w_mix_out.shape[1]
    hbm = pl.BlockSpec(memory_space=pltpu.HBM)
    vmem = pl.BlockSpec(memory_space=pltpu.VMEM)
    dma = pltpu.SemaphoreType.DMA
    n_chunks = len(ff_chunks(n_ff))
    ys, xs, per_chunk = dma((n_y,)), dma((n_tp,)), dma((n_y, n_chunks))
    out_t, new_memory, new_normalizer, new_stabilizer = pl.pallas_call(
        functools.partial(layer_kernel, n_kv, n_tp),
        out_shape=(
            jax.ShapeDtypeStruct((mine, seqs), BF16),
            jax.ShapeDtypeStruct(memory.shape, F32),
            jax.ShapeDtypeStruct(normalizer.shape, F32),
            jax.ShapeDtypeStruct(stabilizer.shape[::-1], F32),
        ),
        in_specs=[hbm, vmem] + [hbm] * 10 + [vmem] + [hbm] * 3,
        out_specs=(vmem, hbm, vmem, vmem),
        scratch_shapes=[
            pltpu.VMEM((feats, n1), BF16),
            pltpu.VMEM((2 * w_input_gate.shape[1], feats), BF16),
            pltpu.VMEM(memory.shape, F32),
            pltpu.VMEM(normalizer.shape, F32),
            pltpu.VMEM(stabilizer.shape[::-1], F32),
            pltpu.VMEM(w_mix_out.shape, BF16),
            pltpu.VMEM(w_mix_out.shape[::-1], BF16),
            pltpu.VMEM((feats, n2), BF16),
            pltpu.VMEM(w_down.shape, BF16),
            pltpu.VMEM(w_down.shape[::-1], BF16),
            pltpu.VMEM((feats, seqs), BF16),
            pltpu.VMEM((n_y, 2, own, feats), BF16),
            pltpu.VMEM((n_y, own, n1), BF16),
            pltpu.VMEM((n_y, own, n1), F32),
            pltpu.VMEM((n_y, own, n1), BF16),
            pltpu.VMEM((n_y, own, n1), BF16),
            pltpu.VMEM((n_y, own, n1), BF16),
            pltpu.VMEM((own, dv), F32),
            pltpu.VMEM((seqs, dv), BF16),
            pltpu.VMEM((n_tp, mine, seqs), BF16),
            pltpu.VMEM((n_tp, mine, seqs), BF16),
            pltpu.VMEM((out_feats, seqs), BF16),
            pltpu.VMEM((n_y, own, n2), BF16),
            pltpu.VMEM((n_y, own, n2), F32),
            pltpu.VMEM((n_y, own, n2), BF16),
            pltpu.VMEM((n_y, own, n2), BF16),
            pltpu.VMEM((n_y, own, n2), BF16),
            pltpu.VMEM((seqs, n_ff), BF16),
            pltpu.VMEM((out_feats, seqs), F32),
            pltpu.VMEM((n_tp, mine, seqs), BF16),
            pltpu.VMEM((n_tp, mine, seqs), BF16),
            dma((13 + 2 * len(ff_chunks(n_ff)),)),
            xs, xs,
            dma((3,)), dma((3,)), dma((n_y, 3)), dma((n_y, 3)),
            ys, ys, ys, ys,
            xs, xs,
            xs, xs,
            dma((n_chunks,)), dma((n_chunks,)), per_chunk, per_chunk,
            per_chunk, per_chunk, per_chunk, per_chunk,
            xs, xs,
        ],
        compiler_params=pltpu.CompilerParams(collective_id=0, has_side_effects=True, vmem_limit_bytes=67_043_328),
        name="layer",
    )(
        tokens.T, norm_gain, w_query, w_key, w_value, w_outgate, w_input_gate.T, w_forget_gate.T,
        memory, normalizer, stabilizer.T, w_mix_out, ffn_gain, w_gate, w_up, w_down,
    )
    out_t, new_memory, new_normalizer, new_stabilizer = hand_over(out_t, new_memory, new_normalizer, new_stabilizer)
    return out_t.T, new_memory, new_normalizer, new_stabilizer.T


def solution(mesh):
    in_specs = (
        P("grp", ("kv", "tp")),
        P("kv"),
        P("kv", "tp"),
        P("kv", "tp"),
        P("kv", "tp"),
        P("kv", "tp"),
        P("kv", None),
        P("kv", None),
        P(("grp", "kv"), "tp", None, None),
        P(("grp", "kv"), "tp", None),
        P(("grp", "kv"), "tp"),
        P("tp", "kv"),
        P("kv"),
        P("kv", "tp"),
        P("kv", "tp"),
        P("tp", "kv"),
    )
    out_specs = (
        P("grp", ("kv", "tp")),
        P(("grp", "kv"), "tp", None, None),
        P(("grp", "kv"), "tp", None),
        P(("grp", "kv"), "tp"),
    )
    body = functools.partial(shards, mesh.shape["kv"], mesh.shape["tp"])
    return jax.shard_map(body, mesh=mesh, in_specs=in_specs, out_specs=out_specs, check_vma=False)
```
